128 devices in a mesh: ep: 128 (over z, y, x, core).
Axes of the slice: x: 4, y: 4, z: 4, core: 2. Of those that a mesh axis runs over, the one named last changes fastest.
Arguments:
- tokens: bfloat16 [1024, 2048], P('ep'), may hold values from -6 to 6
- cache_keys: bfloat16 [1024, 1024, 128], P('ep'), may hold values from -80 to 80
- cache_values: bfloat16 [1024, 1024, 128], P('ep'), may hold values from -6 to 6
- cum_gates: float32 [1024, 1024, 2], P('ep'), may hold values from -1024 to 0, as said below
- lengths: int32 [1024], P('ep'), may hold values from 128 to 1024
- query_weight: bfloat16 [2048, 2048], replicated, may hold values from -0.125 to 0.125
- key_weight: bfloat16 [2048, 128], replicated, may hold values from -0.125 to 0.125
- value_weight: bfloat16 [2048, 128], replicated, may hold values from -0.125 to 0.125
- forget_weight: bfloat16 [2048, 2], replicated, may hold values from -0.125 to 0.125
- out_weight: bfloat16 [2048, 2048], P('ep'), may hold values from -1 to 1
- norm_gain: float32 [2, 2048], replicated, may hold values from 0.1 to 1.9
- norm_bias: float32 [2, 2048], replicated, may hold values from -1 to 1
- dense_gate_weight: bfloat16 [2048, 5632], P(None, 'ep'), may hold values from -0.125 to 0.125
- dense_up_weight: bfloat16 [2048, 5632], P(None, 'ep'), may hold values from -0.125 to 0.125
- dense_down_weight: bfloat16 [5632, 2048], P('ep'), may hold values from -0.078125 to 0.078125
- dense_scale: float32 [2048], replicated, may hold values from 0.2 to 1.5
- expert_gate_weight: bfloat16 [2048, 57344], P(None, 'ep'), may hold values from -0.125 to 0.125
- expert_up_weight: bfloat16 [2048, 57344], P(None, 'ep'), may hold values from -0.125 to 0.125
- expert_down_weight: bfloat16 [57344, 2048], P('ep'), may hold values from -0.0625 to 0.0625
- routes: int32 [1024, 2], replicated, may hold values from 0 to 7, all different within a row; in each aligned block of 8 rows (0 to 7, 8 to 15, ...) at most 3 rows name the same one
- route_weights: float32 [1024, 2], replicated, may hold values from 0.2 to 1
Outputs:
- output: bfloat16 [1024, 2048], P('ep')
The draws below stay inside these ranges and needn't reach their ends.
Inputs may be any that keep to these rules, and one draw needn't show every extreme that they name: `routes`: each row names 2 different experts; the rows of one device (8 aligned rows) name one expert at most 3 times. `cum_gates`: non-increasing along positions.
All inputs are finite; a program needn't handle non-finite values.
Results may differ from the reference program's by a relative error of at most 0.012.
Values may be sent and summed in bfloat16 or wider, within the bound.
A program may use at most 128 MiB of HBM per device.

```python
import math
import jax
import jax.numpy as jnp
import numpy as np
from jax import lax

D = 2048
HEADS = 32
HEAD_DIM = 64
KEY_VALUE_HEADS = 2
FF_DENSE = 5632
FF_EXPERT = 7168
EXPERTS = 8
TOP = 2
SEQ_DEV = 8
CACHE_SLOTS = 1024
SEQUENCE_COUNT = 1024
CAP = 3
N_EP = 128


def draw_cache_keys(key, part):
    key_rows = jax.random.split(key, 1)
    shape = (SEQUENCE_COUNT, CACHE_SLOTS, KEY_VALUE_HEADS * HEAD_DIM)
    return jax.random.normal(key_rows[0], shape, jnp.float32).astype(jnp.bfloat16)


def draw_cum_gates(key, part):
    key_rows = jax.random.split(key, 7)
    devices = SEQUENCE_COUNT // SEQ_DEV
    share_fast = 0.5
    fast = jax.random.uniform(key_rows[0], (SEQUENCE_COUNT, 1, KEY_VALUE_HEADS)) < share_fast
    fast_rate = jnp.exp(jax.random.uniform(key_rows[1], (SEQUENCE_COUNT, 1, KEY_VALUE_HEADS), jnp.float32, math.log(1.0 / 100.0), math.log(1.0 / 30.0)))
    slow_rate = jnp.exp(jax.random.uniform(key_rows[2], (SEQUENCE_COUNT, 1, KEY_VALUE_HEADS), jnp.float32, math.log(0.1), math.log(0.4))) / CACHE_SLOTS
    decay_rate = jnp.where(fast, fast_rate, slow_rate)
    per_device_ratio = jnp.exp(jax.random.uniform(key_rows[3], (devices, 1, 1), jnp.float32, 0.0, math.log(3.0)))
    per_device_ratio = jnp.repeat(per_device_ratio, SEQ_DEV, axis=0)
    coarse_estimate = jnp.exp(jax.random.uniform(key_rows[4], (SEQUENCE_COUNT, CACHE_SLOTS, KEY_VALUE_HEADS), jnp.float32, math.log(0.5), math.log(2.0)))
    spike_position = jax.random.randint(key_rows[5], (SEQUENCE_COUNT, 1, KEY_VALUE_HEADS, 2), 0, CACHE_SLOTS)
    decay_penalty = jax.random.uniform(key_rows[6], (SEQUENCE_COUNT, 1, KEY_VALUE_HEADS, 2), jnp.float32, 0.2, 0.5)
    current_slot = jnp.arange(CACHE_SLOTS, dtype=jnp.int32)[None, :, None, None]
    spike_amount = jnp.sum(jnp.where(current_slot == spike_position, -jnp.log(1.0 - decay_penalty), 0.0), axis=3)
    step_total = decay_rate * per_device_ratio * coarse_estimate + spike_amount
    return jnp.cumsum(-step_total, axis=1).astype(jnp.float32)


def with_ends(result, key, least, largest):
    longest = result.shape.index(max(result.shape))
    spots = []
    for shift in (0, 1):
        where = [jax.random.randint(jax.random.fold_in(key, axis), (), 0, length) for axis, length in enumerate(result.shape)]
        where[longest] = (where[longest] + shift) % result.shape[longest]
        spots.append(tuple(where))
    return result.at[spots[0]].set(least).at[spots[1]].set(largest)


def levels(stream_key, dims, cuts, smallest, top_value):
    level, own = 1.0, jax.random.fold_in(stream_key, 6)
    for dim, parts in cuts:
        heights = jnp.exp(jax.random.uniform(jax.random.fold_in(own, dim), (parts,), jnp.float32, smallest / len(cuts), top_value / len(cuts)))
        level = level * jnp.repeat(heights, dims[dim] // parts).reshape([-1 if axis == dim else 1 for axis in range(len(dims))])
    return level


def routed_block(stream_key, own, number, rows, count, top, reach, slope):
    ranking = jax.random.permutation(stream_key, count)
    crowded, common = load_shares(count, rows * top, reach, slope, True), load_shares(count, rows * top, reach, slope, False)
    places = jnp.arange(count)

    def named(tallies, turn):
        used = int((tallies > 0).sum())
        fixed = max(1, used // 4)
        shifted = fixed + (places - fixed + turn * (used - fixed)) % max(1, count - fixed)
        return jnp.zeros((count,), jnp.int32).at[ranking[jnp.where(places < fixed, places, shifted)]].set(jnp.asarray(tallies, jnp.int32))

    tallies = jnp.where(number % 4 == 0, named(crowded, number // 4), named(common, number - number // 4 - 1))
    mixed = jax.random.permutation(jax.random.fold_in(own, 3), count)
    source_of, taker = mixed[0:count // 2 * 2:2], mixed[1:count // 2 * 2:2]
    slack = jnp.minimum(tallies[source_of] - 1, reach - tallies[taker]) // 2
    slack = jnp.where((source_of == ranking[0]) | (taker == ranking[0]) | (tallies[taker] == 0), 0, jnp.maximum(slack, 0))
    shifted = jax.random.randint(jax.random.fold_in(own, 4), (count // 2,), 0, 1 << 20) % (slack + 1)
    tallies = tallies.at[source_of].add(-shifted).at[taker].add(shifted)
    items = jnp.searchsorted(jnp.cumsum(tallies), jnp.arange(rows * top), side="right").astype(jnp.int32)
    table = items.reshape(top, rows).T
    table = table[jax.random.permutation(jax.random.fold_in(own, 1), rows)]
    turn = jax.random.randint(jax.random.fold_in(own, 2), (rows, 1), 0, top)
    return jnp.take_along_axis(table, (jnp.arange(top)[None, :] + turn) % top, axis=1)


def load_shares(count, total, bound, skew, full):
    weights = [(1 << 20) // math.isqrt(rank ** skew) + 1 for rank in range(1, count + 1)]
    largest = bound if full else min(bound, max(-(-total // count), total * weights[0] // sum(weights)))
    least = 1 if total - largest >= count - 1 else 0
    holding, spare = [largest] + [least] * (count - 1), total - largest - least * (count - 1)
    while spare > 0:
        movable = [i for i in range(1, count) if holding[i] < largest] or [i for i in range(1, count) if holding[i] < bound]
        whole, remaining = sum([weights[i] for i in movable]), spare
        for i in movable:
            more = min(bound - holding[i], max(1, remaining * weights[i] // whole), spare)
            holding[i] = holding[i] + more
            spare = spare - more
    return np.array(holding)


def normal_values(stream_key, shape, scale, reach, cuts=(), held_as=jnp.bfloat16):
    level = levels(stream_key, shape, cuts, -0.22, 0.18) if cuts else 1.0
    values = jax.random.normal(stream_key, shape, jnp.float32) * scale * level
    return jnp.minimum(jnp.maximum(values, -reach), reach).astype(held_as)


def setup_inputs(seed: int = 0) -> dict:
    keys = jax.random.split(jax.random.key(seed), 22)
    tokens = normal_values(keys[0], (SEQUENCE_COUNT, D), 1.0, 6.0, ((0, 128),))
    cache_keys = draw_cache_keys(jax.random.fold_in(keys[21], 71), 0)
    cache_values = normal_values(keys[2], (SEQUENCE_COUNT, CACHE_SLOTS, KEY_VALUE_HEADS * HEAD_DIM), 1.0, 6.0, ((0, 128),))
    cum_gates = draw_cum_gates(jax.random.fold_in(keys[21], 71), 0)
    lengths = with_ends(jax.random.randint(keys[4], (SEQUENCE_COUNT,), CACHE_SLOTS // 8, CACHE_SLOTS + 1), jax.random.fold_in(keys[4], 1), CACHE_SLOTS // 8, CACHE_SLOTS).astype(jnp.int32)
    query_weight = normal_values(keys[5], (D, HEADS * HEAD_DIM), D ** -0.5, 0.125)
    key_weight = normal_values(keys[6], (D, KEY_VALUE_HEADS * HEAD_DIM), D ** -0.5, 0.125)
    value_weight = normal_values(keys[7], (D, KEY_VALUE_HEADS * HEAD_DIM), D ** -0.5, 0.125)
    forget_weight = normal_values(keys[8], (D, KEY_VALUE_HEADS), D ** -0.5, 0.125)
    out_weight = normal_values(keys[9], (HEADS * HEAD_DIM, D), (HEADS * HEAD_DIM // 64) ** -0.5, 1.0, ((0, 128),))
    norm_gain = jnp.clip(1.0 + 0.18 * jax.random.normal(keys[10], (2, D), jnp.float32), 0.1, 1.9)
    norm_bias = normal_values(keys[11], (2, D), 0.2, 1.0, (), jnp.float32)
    dense_gate_weight = normal_values(keys[12], (D, FF_DENSE), D ** -0.5, 0.125, ((1, 128),))
    dense_up_weight = normal_values(keys[13], (D, FF_DENSE), D ** -0.5, 0.125, ((1, 128),))
    dense_down_weight = normal_values(keys[14], (FF_DENSE, D), FF_DENSE ** -0.5, 0.078125, ((0, 128),))
    dense_scale = jnp.clip(jax.random.uniform(keys[15], (D,), jnp.float32, 0.2, 1.5), 0.2, 1.5)
    expert_gate_weight = normal_values(keys[16], (D, EXPERTS * FF_EXPERT), D ** -0.5, 0.125, ((1, 128),))
    expert_up_weight = normal_values(keys[17], (D, EXPERTS * FF_EXPERT), D ** -0.5, 0.125, ((1, 128),))
    expert_down_weight = normal_values(keys[18], (EXPERTS * FF_EXPERT, D), FF_EXPERT ** -0.5, 0.0625, ((0, 128),))
    routes_keys = jax.random.split(jax.random.fold_in(keys[19], 1), SEQUENCE_COUNT // SEQ_DEV)
    routes_turns = jax.random.permutation(jax.random.fold_in(keys[19], 3), SEQUENCE_COUNT // SEQ_DEV)
    routes = jax.vmap(lambda own, number: routed_block(jax.random.fold_in(keys[19], 2), own, number, SEQ_DEV, EXPERTS, TOP, CAP, 2))(routes_keys, routes_turns).reshape((SEQUENCE_COUNT, TOP))
    route_weights = jnp.clip(jax.random.uniform(keys[20], (SEQUENCE_COUNT, TOP), jnp.float32, 0.2, 1.0), 0.2, 1.0)
    return dict(tokens=tokens, cache_keys=cache_keys, cache_values=cache_values, cum_gates=cum_gates, lengths=lengths, query_weight=query_weight, key_weight=key_weight, value_weight=value_weight, forget_weight=forget_weight, out_weight=out_weight, norm_gain=norm_gain, norm_bias=norm_bias, dense_gate_weight=dense_gate_weight, dense_up_weight=dense_up_weight, dense_down_weight=dense_down_weight, dense_scale=dense_scale, expert_gate_weight=expert_gate_weight, expert_up_weight=expert_up_weight, expert_down_weight=expert_down_weight, routes=routes, route_weights=route_weights)


residual_scale = 1.4142135
norm_eps = 1e-05

def layer_norm(values, gain_row, shift_row):
    centre = lax.optimization_barrier(jnp.mean(values, axis=-1, keepdims=True))
    centred = values - centre
    spread = lax.optimization_barrier(jnp.mean(centred * centred, axis=-1, keepdims=True))
    return (centred * lax.rsqrt(spread + norm_eps) * gain_row + shift_row).astype(jnp.bfloat16)

def attend_block(inputs):
    queries, cached_keys, cached_values, gate_sums, length_row, fresh_key, fresh_value, fresh_gate = inputs
    amount = queries.shape[0]
    grouped = HEADS // KEY_VALUE_HEADS
    query_grid_four = queries.astype(jnp.float32).reshape(amount, KEY_VALUE_HEADS, grouped, HEAD_DIM)
    key_four = cached_keys.astype(jnp.float32).reshape(amount, CACHE_SLOTS, KEY_VALUE_HEADS, HEAD_DIM)
    value_four = cached_values.astype(jnp.float32).reshape(amount, CACHE_SLOTS, KEY_VALUE_HEADS, HEAD_DIM)
    self_key_row = fresh_key.astype(jnp.float32).reshape(amount, KEY_VALUE_HEADS, HEAD_DIM)
    own_value = fresh_value.astype(jnp.float32).reshape(amount, KEY_VALUE_HEADS, HEAD_DIM)
    ratio_value = HEAD_DIM ** (-0.5)
    latest = jnp.take_along_axis(gate_sums, (length_row - 1).astype(jnp.int32)[:, None, None], axis=1)
    offsets = jnp.transpose(latest - gate_sums + fresh_gate[:, None, :], (0, 2, 1))
    past = jnp.einsum('bkgd,blkd->bkgl', query_grid_four, key_four) * ratio_value + offsets[:, :, None, :]
    live = jnp.arange(CACHE_SLOTS, dtype=jnp.int32)[None, :] < length_row[:, None]
    past = jnp.where(live[:, None, None, :], past, -jnp.inf)
    self_part = jnp.einsum('rifs,ris->rif', query_grid_four, self_key_row) * ratio_value
    highest = jnp.maximum(lax.optimization_barrier(jnp.max(past, axis=-1)), self_part)
    past_exp = jnp.exp(past - highest[..., None])
    own_exp = jnp.exp(self_part - highest)
    denominator = lax.optimization_barrier(jnp.sum(past_exp, axis=-1)) + own_exp
    past_weight = lax.optimization_barrier((past_exp / denominator[..., None]).astype(jnp.bfloat16)).astype(jnp.float32)
    own_weight = lax.optimization_barrier((own_exp / denominator).astype(jnp.bfloat16)).astype(jnp.float32)
    mixed = jnp.einsum('bkgl,blkd->bkgd', past_weight, value_four) + own_weight[..., None] * own_value[:, :, None, :]
    return mixed.reshape(amount, HEADS * HEAD_DIM).astype(jnp.bfloat16)

def expert_mix(settled, expert_gate, expert_up, expert_down, routes, route_weights):
    shards = N_EP // EXPERTS
    part_width = FF_EXPERT // shards
    chosen = routes.reshape(N_EP, SEQ_DEV, TOP)
    shares = route_weights.reshape(N_EP, SEQ_DEV, TOP)
    expert_ids = jnp.arange(EXPERTS, dtype=jnp.int32)
    picked = (chosen[..., None] == expert_ids).astype(jnp.int32)
    hits = lax.optimization_barrier(jnp.sum(picked, axis=2))
    portion = lax.optimization_barrier(jnp.sum(picked.astype(jnp.float32) * shares[..., None], axis=2))
    ranks = jnp.cumsum(hits, axis=1) - hits
    slot_ids = jnp.arange(CAP, dtype=jnp.int32)
    matched = (hits[..., None] * (ranks[..., None] == slot_ids).astype(jnp.int32)).astype(jnp.float32)
    by_source = settled.astype(jnp.float32).reshape(N_EP, SEQ_DEV, D)

    def one_expert(running, expert):
        select = lax.dynamic_index_in_dim(matched, expert, 2, keepdims=False)
        weight_here = lax.dynamic_index_in_dim(portion, expert, 2, keepdims=False)
        slot_rows = jnp.einsum('nsc,nsd->ncd', select, by_source, precision=lax.Precision.HIGHEST)
        slot_rows = slot_rows.reshape(N_EP * CAP, D).astype(jnp.bfloat16)
        gate_cols = lax.dynamic_slice_in_dim(expert_gate, expert * FF_EXPERT, FF_EXPERT, 1)
        up_cols = lax.dynamic_slice_in_dim(expert_up, expert * FF_EXPERT, FF_EXPERT, 1)
        down_rows = lax.dynamic_slice_in_dim(expert_down, expert * FF_EXPERT, FF_EXPERT, 0)
        gate_val = jnp.dot(slot_rows, gate_cols, preferred_element_type=jnp.float32)
        up_val = jnp.dot(slot_rows, up_cols, preferred_element_type=jnp.float32)
        hidden = (jax.nn.silu(gate_val) * up_val).astype(jnp.bfloat16)
        pieces = jnp.einsum('rgf,gfd->rgd', hidden.astype(jnp.float32).reshape(N_EP * CAP, shards, part_width), down_rows.astype(jnp.float32).reshape(shards, part_width, D))
        pieces = lax.optimization_barrier(pieces.astype(jnp.bfloat16)).astype(jnp.float32)
        summed = lax.optimization_barrier(jnp.sum(pieces, axis=1)).reshape(N_EP, CAP, D)
        placed = jnp.einsum('nsc,ncd->nsd', select, summed, precision=lax.Precision.HIGHEST)
        return (running + weight_here[..., None] * placed, None)
    combined, unused = lax.scan(one_expert, jnp.zeros((N_EP, SEQ_DEV, D), jnp.float32), jnp.arange(EXPERTS, dtype=jnp.int32))
    return combined.reshape(N_EP * SEQ_DEV, D)

def reference(tokens, cache_keys, cache_values, cum_gates, lengths, query_weight, key_weight, value_weight, forget_weight, out_weight, norm_gain, norm_bias, dense_gate_weight, dense_up_weight, dense_down_weight, dense_scale, expert_gate_weight, expert_up_weight, expert_down_weight, routes, route_weights):
    query = jnp.dot(tokens, query_weight, preferred_element_type=jnp.float32).astype(jnp.bfloat16)
    new_key = jnp.dot(tokens, key_weight, preferred_element_type=jnp.float32).astype(jnp.bfloat16)
    new_value = jnp.dot(tokens, value_weight, preferred_element_type=jnp.float32).astype(jnp.bfloat16)
    new_gate = jax.nn.log_sigmoid(jnp.dot(tokens, forget_weight, preferred_element_type=jnp.float32))

    def blocks(array):
        return array.reshape((N_EP, SEQ_DEV) + array.shape[1:])
    attended = lax.map(attend_block, (blocks(query), blocks(cache_keys), blocks(cache_values), blocks(cum_gates), blocks(lengths), blocks(new_key), blocks(new_value), blocks(new_gate)))
    attended = attended.reshape(SEQUENCE_COUNT, HEADS * HEAD_DIM)
    projected = jnp.dot(attended, out_weight, preferred_element_type=jnp.float32)
    settled = layer_norm(residual_scale * tokens.astype(jnp.float32) + projected, norm_gain[0], norm_bias[0])
    dense_gate = jnp.dot(settled, dense_gate_weight, preferred_element_type=jnp.float32)
    dense_up = jnp.dot(settled, dense_up_weight, preferred_element_type=jnp.float32)
    dense_hidden = (jax.nn.silu(dense_gate) * dense_up).astype(jnp.bfloat16)
    dense_out = jnp.dot(dense_hidden, dense_down_weight, preferred_element_type=jnp.float32)
    expert_out = expert_mix(settled, expert_gate_weight, expert_up_weight, expert_down_weight, routes, route_weights)
    ffn = expert_out + dense_scale * dense_out
    return layer_norm(residual_scale * settled.astype(jnp.float32) + ffn, norm_gain[1], norm_bias[1])
```

```python
import functools

import jax
import jax.numpy as jnp
from jax import lax
from jax.experimental import pallas as pl
from jax.experimental.pallas import tpu as pltpu
from jax.sharding import PartitionSpec as P

MESH = pl.DeviceIdType.MESH
F32 = jnp.float32
BF16 = jnp.bfloat16
SIDE = 4
ROWS = 8
WIDTH = 2048
EXPERTS = 8
FFE = 448
FFD = 44
FFP = 512
CHUNKS = ((0, 768), (768, 640), (1408, 640))
GATHER_ORDER = ((2, 1, 0), (0, 2, 1), (1, 0, 2))
residual_scale = 1.4142135
norm_eps = 1e-05


def norm_rows(values, gain_row, shift_row):
    centre = jnp.mean(values, axis=-1, keepdims=True)
    centred = values - centre
    spread = jnp.mean(centred * centred, axis=-1, keepdims=True)
    return (centred * lax.rsqrt(spread + norm_eps) * gain_row + shift_row).astype(BF16)


def position():
    me = lax.axis_index("ep")
    core = me % 2
    x = (me // 2) % SIDE
    y = (me // (2 * SIDE)) % SIDE
    z = me // (2 * SIDE * SIDE)
    return core, (z, y, x)


def device_at(core, spot):
    z, y, x = spot
    return (((z * SIDE + y) * SIDE + x) * 2 + core,)


def moved(spot, dim, value):
    return tuple(value if d == dim else spot[d] for d in range(3))


def shifted(spot, dim, offset):
    return moved(spot, dim, (spot[dim] + offset + SIDE) % SIDE)


def columns(k):
    return pl.ds(CHUNKS[k][0], CHUNKS[k][1])


def remote(src, dst, send, recv, target):
    return pltpu.make_async_remote_copy(
        src_ref=src, dst_ref=dst, send_sem=send, recv_sem=recv, device_id=target, device_id_type=MESH
    )


def entry_barrier(core, spot):
    barrier = pltpu.get_barrier_semaphore()
    pl.semaphore_signal(barrier, inc=1, device_id=device_at(1 - core, spot), device_id_type=MESH)
    for dim in range(3):
        for offset in range(1, SIDE):
            pl.semaphore_signal(
                barrier, inc=1, device_id=device_at(core, shifted(spot, dim, offset)), device_id_type=MESH
            )
    pl.semaphore_wait(barrier, 3 * (SIDE - 1) + 1)


def gather_region(rows_ref, k, core, spot, done):
    where = tuple(pl.ds(0, SIDE) if d in done else spot[d] for d in range(3))
    return rows_ref.at[(core,) + where + (pl.ds(0, ROWS), columns(k))]


def gather_rows(rows_ref, core, spot, gsend, grecv, fsend, frecv, osend, orecv):
    started = []
    partner = device_at(1 - core, spot)
    own = rows_ref.at[(core,) + spot]
    copy = remote(own, own, osend, orecv, partner)
    copy.start()
    started.append(copy)

    def start(k, phase):
        order = GATHER_ORDER[k]
        region = gather_region(rows_ref, k, core, spot, order[:phase])
        for offset in range(1, SIDE):
            target = device_at(core, shifted(spot, order[phase], offset))
            copy = remote(
                region, region, gsend.at[k, phase, offset - 1], grecv.at[k, phase, offset - 1], target
            )
            copy.start()
            started.append(copy)

    def arrive(k, phase):
        order = GATHER_ORDER[k]
        for offset in range(1, SIDE):
            source = shifted(spot, order[phase], -offset)
            region = gather_region(rows_ref, k, core, source, order[:phase])
            remote(
                region, region, gsend.at[k, phase, offset - 1], grecv.at[k, phase, offset - 1],
                device_at(core, source),
            ).wait_recv()

    def forward(k, phase):
        order = GATHER_ORDER[k]
        for offset in range(1, SIDE):
            source = shifted(spot, order[phase], -offset)
            region = gather_region(rows_ref, k, core, source, order[:phase])
            copy = remote(
                region, region, fsend.at[k, phase, offset - 1], frecv.at[k, phase, offset - 1], partner
            )
            copy.start()
            started.append(copy)

    def forwarded(k, phase):
        order = GATHER_ORDER[k]
        for offset in range(1, SIDE):
            source = shifted(spot, order[phase], -offset)
            region = gather_region(rows_ref, k, 1 - core, source, order[:phase])
            remote(
                region, region, fsend.at[k, phase, offset - 1], frecv.at[k, phase, offset - 1], partner
            ).wait_recv()

    for k in range(3):
        start(k, 0)
    for phase in range(3):
        for k in range(3):
            arrive(k, phase)
            if phase < 2:
                start(k, phase + 1)
            forward(k, phase)
    other = rows_ref.at[(1 - core,) + spot]
    remote(other, other, osend, orecv, partner).wait_recv()
    for phase in range(3):
        for k in range(3):
            forwarded(k, phase)
    return started


def left_over(k, phase):
    gone = GATHER_ORDER[k][::-1][:phase]
    return [d for d in range(3) if d not in gone]


def ffn_kernel(
    settled_ref, routes_ref, shares_ref, gate_hbm, up_hbm, down_hbm, dgate_ref, dup_ref, ddown_ref,
    scale_ref, gain_ref, bias_ref, out_ref,
    rows_ref, wg_ref, wu_ref, wd_ref, factor_ref, part_ref, twin_ref, r0_ref, r1_ref, r2_ref, s1_ref, s2_ref,
    wsem, gsend, grecv, fsend, frecv, osend, orecv, tsend, trecv, rsend, rrecv,
):
    core, spot = position()
    entry_barrier(core, spot)
    loads = [
        pltpu.make_async_copy(gate_hbm, wg_ref.at[pl.ds(0, FFE)], wsem.at[0]),
        pltpu.make_async_copy(up_hbm, wu_ref.at[pl.ds(0, FFE)], wsem.at[1]),
        pltpu.make_async_copy(down_hbm, wd_ref.at[pl.ds(0, FFE)], wsem.at[2]),
    ]
    for load in loads:
        load.start()
    rows_ref[(core,) + spot] = settled_ref[...]
    pad = jnp.zeros((FFP - FFE - FFD, WIDTH), BF16)
    for ref, dense in ((wg_ref, dgate_ref[...]), (wu_ref, dup_ref[...])):
        ref[FFE:, :] = jnp.concatenate([dense, pad], axis=0)
    ddown = (ddown_ref[...].astype(F32) * scale_ref[...]).astype(BF16)
    wd_ref[FFE:, :] = jnp.concatenate([ddown, pad], axis=0)
    expert = lax.axis_index("ep") // (2 * SIDE * SIDE * SIDE // EXPERTS)
    picked = jnp.where(routes_ref[...] == expert, shares_ref[...], 0.0)
    factor = jnp.sum(picked, axis=0, keepdims=True)
    turned = jnp.transpose(jnp.broadcast_to(factor, (8, factor.shape[1])))
    factor_ref[...] = turned.reshape(factor_ref.shape)

    started = gather_rows(rows_ref, core, spot, gsend, grecv, fsend, frecv, osend, orecv)
    for load in loads:
        load.wait()

    nt = (((1,), (1,)), ((), ()))
    block = 2 * SIDE * SIDE * ROWS
    lane = lax.broadcasted_iota(jnp.int32, (1, FFP), 1)

    def part_of(half, plane):
        x = rows_ref.at[half, pl.ds(plane, 2)].reshape(block, WIDTH)[...]
        gate = lax.dot_general(x, wg_ref[...], nt, preferred_element_type=F32)
        up = lax.dot_general(x, wu_ref[...], nt, preferred_element_type=F32)
        weight = factor_ref[pl.ds(plane * SIDE * SIDE, 2 * SIDE * SIDE), half].reshape(block, 8)[:, :1]
        weight = jnp.where(lane < FFE, weight, 1.0)
        hidden = (gate * jax.nn.sigmoid(gate) * up * weight).astype(BF16)
        return jnp.dot(hidden, wd_ref[...], preferred_element_type=F32)

    partner = device_at(1 - core, spot)

    def twin_copy(i):
        return remote(
            part_ref.at[1 - core, pl.ds(2 * i, 2)], twin_ref.at[pl.ds(2 * i, 2)], tsend.at[i], trecv.at[i], partner
        )

    def far(i, carry):
        part_ref.at[1 - core, pl.ds(2 * i, 2)].reshape(block, WIDTH)[...] = part_of(1 - core, 2 * i).astype(BF16)
        twin_copy(i).start()
        return carry

    lax.fori_loop(0, SIDE // 2, far, 0)

    def near(i, carry):
        value = part_of(core, 2 * i)
        twin_copy(i).wait_recv()
        value = value + twin_ref.at[pl.ds(2 * i, 2)].reshape(block, WIDTH)[...].astype(F32)
        part_ref.at[core, pl.ds(2 * i, 2)].reshape(block, WIDTH)[...] = value.astype(BF16)
        return carry

    lax.fori_loop(0, SIDE // 2, near, 0)

    sums = ((part_ref, r0_ref, s1_ref), (s1_ref, r1_ref, s2_ref), (s2_ref, r2_ref, None))

    def slab(ref, phase, k, value):
        dims = left_over(k, phase)
        dim = GATHER_ORDER[k][::-1][phase]
        where = tuple(value if d == dim else pl.ds(0, SIDE) for d in dims)
        if phase == 0:
            where = (core,) + where
        return ref.at[where + (pl.ds(0, ROWS), columns(k))]

    def landed(ref, phase, k, index):
        where = (index,) + tuple(pl.ds(0, SIDE) for _ in range(2 - phase))
        return ref.at[where + (pl.ds(0, ROWS), columns(k))]

    def reduce_copy(phase, k, offset):
        dim = GATHER_ORDER[k][::-1][phase]
        target = shifted(spot, dim, offset)
        return remote(
            slab(sums[phase][0], phase, k, target[dim]), landed(sums[phase][1], phase, k, offset - 1),
            rsend.at[k, phase, offset - 1], rrecv.at[k, phase, offset - 1], device_at(core, target),
        )

    def reduce_start(phase, k):
        for offset in range(1, SIDE):
            copy = reduce_copy(phase, k, offset)
            copy.start()
            started.append(copy)

    def reduce_sum(phase, k):
        dim = GATHER_ORDER[k][::-1][phase]
        total = slab(sums[phase][0], phase, k, spot[dim])[...].astype(F32)
        for offset in range(1, SIDE):
            reduce_copy(phase, k, offset).wait_recv()
            total = total + landed(sums[phase][1], phase, k, offset - 1)[...].astype(F32)
        return total

    for k in range(3):
        reduce_start(0, k)
    for phase in range(2):
        for k in range(3):
            where = tuple(pl.ds(0, SIDE) for _ in range(2 - phase)) + (pl.ds(0, ROWS), columns(k))
            sums[phase][2][where] = reduce_sum(phase, k).astype(BF16)
            reduce_start(phase + 1, k)
    ffn = jnp.concatenate([reduce_sum(2, k) for k in range(3)], axis=-1)
    out_ref[...] = norm_rows(
        residual_scale * settled_ref[...].astype(F32) + ffn, gain_ref[1:2, :], bias_ref[1:2, :]
    )
    for copy in started:
        copy.wait_send()
    for i in range(SIDE // 2):
        twin_copy(i).wait_send()


def ffn_call(settled, routes, shares, gate, up, down, dgate, dup, ddown, scale, gain, bias):
    vmem = pl.BlockSpec(memory_space=pltpu.VMEM)
    hbm = pl.BlockSpec(memory_space=pltpu.HBM)
    sem = pltpu.SemaphoreType.DMA
    cube = (SIDE, SIDE, SIDE, ROWS, WIDTH)
    return pl.pallas_call(
        ffn_kernel,
        out_shape=jax.ShapeDtypeStruct((ROWS, WIDTH), BF16),
        in_specs=[vmem, vmem, vmem, hbm, hbm, hbm, vmem, vmem, vmem, vmem, vmem, vmem],
        out_specs=vmem,
        scratch_shapes=[
            pltpu.VMEM((2,) + cube, BF16),
            pltpu.VMEM((FFP, WIDTH), BF16),
            pltpu.VMEM((FFP, WIDTH), BF16),
            pltpu.VMEM((FFP, WIDTH), BF16),
            pltpu.VMEM((SIDE**3, 2, ROWS, 8), F32),
            pltpu.VMEM((2,) + cube, BF16),
            pltpu.VMEM(cube, BF16),
            pltpu.VMEM((SIDE - 1,) + cube[1:], BF16),
            pltpu.VMEM((SIDE - 1,) + cube[2:], BF16),
            pltpu.VMEM((SIDE - 1,) + cube[3:], BF16),
            pltpu.VMEM(cube[1:], BF16),
            pltpu.VMEM(cube[2:], BF16),
            sem((3,)),
            sem((3, 3, SIDE - 1)), sem((3, 3, SIDE - 1)),
            sem((3, 3, SIDE - 1)), sem((3, 3, SIDE - 1)),
            sem, sem,
            sem((SIDE // 2,)), sem((SIDE // 2,)),
            sem((3, 3, SIDE - 1)), sem((3, 3, SIDE - 1)),
        ],
        compiler_params=pltpu.CompilerParams(
            collective_id=0, has_side_effects=True, vmem_limit_bytes=60 * 2**20
        ),
        name="ffn",
    )(settled, routes, shares, gate, up, down, dgate, dup, ddown, scale, gain, bias)


def layer_norm(values, gain_row, shift_row):
    return norm_rows(values, gain_row, shift_row)


def attend(
    queries, cached_keys, cached_values, gate_sums, length_row, fresh_key, fresh_value, fresh_gate
):
    amount = queries.shape[0]
    cache_len = cached_keys.shape[1]
    kv_count = fresh_gate.shape[1]
    head_dim = fresh_key.shape[1] // kv_count
    grouped = queries.shape[1] // (kv_count * head_dim)
    query_grid_four = queries.reshape(amount, kv_count, grouped, head_dim)
    key_four = cached_keys.reshape(amount, cache_len, kv_count, head_dim)
    value_four = cached_values.reshape(amount, cache_len, kv_count, head_dim)
    self_key_row = fresh_key.reshape(amount, kv_count, head_dim)
    own_value = fresh_value.astype(jnp.float32).reshape(amount, kv_count, head_dim)
    ratio_value = head_dim ** (-0.5)
    latest = jnp.take_along_axis(gate_sums, (length_row - 1)[:, None, None], axis=1)
    offsets = jnp.transpose(latest - gate_sums + fresh_gate[:, None, :], (0, 2, 1))
    past = jnp.einsum(
        "bkgd,blkd->bkgl", query_grid_four, key_four, preferred_element_type=jnp.float32
    )
    past = past * ratio_value + offsets[:, :, None, :]
    live = jnp.arange(cache_len, dtype=jnp.int32)[None, :] < length_row[:, None]
    past = jnp.where(live[:, None, None, :], past, -jnp.inf)
    self_part = (
        jnp.einsum(
            "rifs,ris->rif", query_grid_four, self_key_row, preferred_element_type=jnp.float32
        )
        * ratio_value
    )
    highest = jnp.maximum(jnp.max(past, axis=-1), self_part)
    past_exp = jnp.exp(past - highest[..., None])
    own_exp = jnp.exp(self_part - highest)
    denominator = jnp.sum(past_exp, axis=-1) + own_exp
    past_weight = (past_exp / denominator[..., None]).astype(jnp.bfloat16)
    own_weight = (own_exp / denominator).astype(jnp.bfloat16)
    mixed = jnp.einsum(
        "bkgl,blkd->bkgd", past_weight, value_four, preferred_element_type=jnp.float32
    )
    mixed = mixed + own_weight.astype(jnp.float32)[..., None] * own_value[:, :, None, :]
    return mixed.reshape(amount, queries.shape[1]).astype(jnp.bfloat16)


def local(
    tokens,
    cache_keys,
    cache_values,
    cum_gates,
    lengths,
    query_weight,
    key_weight,
    value_weight,
    forget_weight,
    out_weight,
    norm_gain,
    norm_bias,
    dense_gate_weight,
    dense_up_weight,
    dense_down_weight,
    dense_scale,
    expert_gate_weight,
    expert_up_weight,
    expert_down_weight,
    routes,
    route_weights,
):
    query = jnp.dot(tokens, query_weight, preferred_element_type=jnp.float32).astype(jnp.bfloat16)
    new_key = jnp.dot(tokens, key_weight, preferred_element_type=jnp.float32).astype(jnp.bfloat16)
    new_value = jnp.dot(tokens, value_weight, preferred_element_type=jnp.float32).astype(
        jnp.bfloat16
    )
    new_gate = jax.nn.log_sigmoid(
        jnp.dot(tokens, forget_weight, preferred_element_type=jnp.float32)
    )
    attended = attend(
        query, cache_keys, cache_values, cum_gates, lengths, new_key, new_value, new_gate
    )
    projected = jnp.dot(
        attended,
        lax.all_gather(out_weight, "ep", axis=0, tiled=True),
        preferred_element_type=jnp.float32,
    )
    settled = layer_norm(
        residual_scale * tokens.astype(jnp.float32) + projected, norm_gain[0], norm_bias[0]
    )
    return ffn_call(
        settled,
        jnp.transpose(routes),
        jnp.transpose(route_weights),
        jnp.transpose(expert_gate_weight),
        jnp.transpose(expert_up_weight),
        expert_down_weight,
        jnp.transpose(dense_gate_weight),
        jnp.transpose(dense_up_weight),
        dense_down_weight,
        dense_scale.reshape(1, -1),
        norm_gain,
        norm_bias,
    )


def solution(mesh):
    return jax.shard_map(
        local,
        mesh=mesh,
        in_specs=(
            P("ep", None),
            P("ep", None, None),
            P("ep", None, None),
            P("ep", None, None),
            P("ep"),
            P(),
            P(),
            P(),
            P(),
            P("ep", None),
            P(),
            P(),
            P(None, "ep"),
            P(None, "ep"),
            P("ep", None),
            P(),
            P(None, "ep"),
            P(None, "ep"),
            P("ep", None),
            P(),
            P(),
        ),
        out_specs=P("ep", None),
        check_vma=False,
    )
```

```python
import functools

import jax
import jax.numpy as jnp
from jax import lax
from jax.experimental import pallas as pl
from jax.experimental.pallas import tpu as pltpu
from jax.sharding import PartitionSpec as P

MESH = pl.DeviceIdType.MESH
F32 = jnp.float32
BF16 = jnp.bfloat16
SIDE = 4
ROWS = 8
WIDTH = 2048
EXPERTS = 8
FFE = 448
FFD = 44
FFP = 512
CHUNKS = ((0, 768), (768, 640), (1408, 640))
GATHER_ORDER = ((2, 1, 0), (0, 2, 1), (1, 0, 2))
ATTEND = 4
residual_scale = 1.4142135
norm_eps = 1e-05


def norm_rows(values, gain_row, shift_row):
    centre = jnp.mean(values, axis=-1, keepdims=True)
    centred = values - centre
    spread = jnp.mean(centred * centred, axis=-1, keepdims=True)
    return (centred * lax.rsqrt(spread + norm_eps) * gain_row + shift_row).astype(BF16)


def position():
    me = lax.axis_index("ep")
    core = me % 2
    x = (me // 2) % SIDE
    y = (me // (2 * SIDE)) % SIDE
    z = me // (2 * SIDE * SIDE)
    return core, (z, y, x)


def device_at(core, spot):
    z, y, x = spot
    return (((z * SIDE + y) * SIDE + x) * 2 + core,)


def moved(spot, dim, value):
    return tuple(value if d == dim else spot[d] for d in range(3))


def shifted(spot, dim, offset):
    return moved(spot, dim, (spot[dim] + offset + SIDE) % SIDE)


def columns(k):
    return pl.ds(CHUNKS[k][0], CHUNKS[k][1])


def remote(src, dst, send, recv, target):
    return pltpu.make_async_remote_copy(
        src_ref=src, dst_ref=dst, send_sem=send, recv_sem=recv, device_id=target, device_id_type=MESH
    )


def entry_barrier(core, spot):
    barrier = pltpu.get_barrier_semaphore()
    pl.semaphore_signal(barrier, inc=1, device_id=device_at(1 - core, spot), device_id_type=MESH)
    for dim in range(3):
        for offset in range(1, SIDE):
            pl.semaphore_signal(
                barrier, inc=1, device_id=device_at(core, shifted(spot, dim, offset)), device_id_type=MESH
            )
    pl.semaphore_wait(barrier, 3 * (SIDE - 1) + 1)


def gather_region(rows_ref, k, core, spot, done):
    where = tuple(pl.ds(0, SIDE) if d in done else spot[d] for d in range(3))
    return rows_ref.at[(core,) + where + (pl.ds(0, ROWS), columns(k))]


def gather_rows(rows_ref, core, spot, gsend, grecv, fsend, frecv, osend, orecv):
    started = []
    partner = device_at(1 - core, spot)
    own = rows_ref.at[(core,) + spot]
    copy = remote(own, own, osend, orecv, partner)
    copy.start()
    started.append(copy)

    def start(k, phase):
        order = GATHER_ORDER[k]
        region = gather_region(rows_ref, k, core, spot, order[:phase])
        for offset in range(1, SIDE):
            target = device_at(core, shifted(spot, order[phase], offset))
            copy = remote(
                region, region, gsend.at[k, phase, offset - 1], grecv.at[k, phase, offset - 1], target
            )
            copy.start()
            started.append(copy)

    def arrive(k, phase):
        order = GATHER_ORDER[k]
        for offset in range(1, SIDE):
            source = shifted(spot, order[phase], -offset)
            region = gather_region(rows_ref, k, core, source, order[:phase])
            remote(
                region, region, gsend.at[k, phase, offset - 1], grecv.at[k, phase, offset - 1],
                device_at(core, source),
            ).wait_recv()

    def forward(k, phase):
        order = GATHER_ORDER[k]
        for offset in range(1, SIDE):
            source = shifted(spot, order[phase], -offset)
            region = gather_region(rows_ref, k, core, source, order[:phase])
            copy = remote(
                region, region, fsend.at[k, phase, offset - 1], frecv.at[k, phase, offset - 1], partner
            )
            copy.start()
            started.append(copy)

    def forwarded(k, phase):
        order = GATHER_ORDER[k]
        for offset in range(1, SIDE):
            source = shifted(spot, order[phase], -offset)
            region = gather_region(rows_ref, k, 1 - core, source, order[:phase])
            remote(
                region, region, fsend.at[k, phase, offset - 1], frecv.at[k, phase, offset - 1], partner
            ).wait_recv()

    for k in range(3):
        start(k, 0)
    for phase in range(3):
        for k in range(3):
            arrive(k, phase)
            if phase < 2:
                start(k, phase + 1)
            forward(k, phase)
    other = rows_ref.at[(1 - core,) + spot]
    remote(other, other, osend, orecv, partner).wait_recv()
    for phase in range(3):
        for k in range(3):
            forwarded(k, phase)
    return started


def left_over(k, phase):
    gone = GATHER_ORDER[k][::-1][:phase]
    return [d for d in range(3) if d not in gone]


PROJ = 512
HALF = 256
WEIGHT_ORDER = ((1, 0), (0, 1))
NT = (((1,), (1,)), ((), ()))
GROUP = 4
HEAD_LANES = 64


def weight_region(wo_ref, k, core, spot, done):
    where = tuple(pl.ds(0, SIDE) if d in done else spot[d] for d in range(2))
    return wo_ref.at[where + (pl.ds(0, SIDE), core, pl.ds(0, 2 * ROWS), pl.ds(k * HALF, HALF))]


class WeightGather:
    def __init__(self, ow_hbm, wo_ref, core, spot, own, wsend, wrecv, xsend, xrecv, fsend, frecv, hsend, hrecv):
        self.ow, self.wo, self.core, self.spot, self.own = ow_hbm, wo_ref, core, spot, own
        self.wsend, self.wrecv, self.xsend, self.xrecv = wsend, wrecv, xsend, xrecv
        self.fsend, self.frecv, self.hsend, self.hrecv = fsend, frecv, hsend, hrecv
        self.partner = device_at(1 - core, spot)
        self.started = []

    def go(self, copy):
        copy.start()
        self.started.append(copy)

    def line_copy(self, offset, source, target):
        z, y, x = source
        first = pl.multiple_of(target[2] * PROJ, PROJ)
        return remote(
            self.ow.at[:, pl.ds(first, PROJ)], self.wo.at[z, y, x, self.core],
            self.xsend.at[offset - 1], self.xrecv.at[offset - 1], device_at(self.core, target),
        )

    def own_copy(self):
        z, y, x = self.spot
        first = pl.multiple_of(x * PROJ, PROJ)
        return pltpu.make_async_copy(self.ow.at[:, pl.ds(first, PROJ)], self.wo.at[z, y, x, self.core], self.own)

    def line_start(self):
        self.own_copy().start()
        for offset in range(1, SIDE):
            self.go(self.line_copy(offset, self.spot, shifted(self.spot, 2, offset)))

    def line_arrive(self):
        self.own_copy().wait()
        for offset in range(1, SIDE):
            self.line_copy(offset, shifted(self.spot, 2, -offset), self.spot).wait_recv()
        self.go(self.line_forward(self.core))

    def line_forward(self, core):
        z, y, x = self.spot
        region = self.wo.at[z, y, pl.ds(0, SIDE), core]
        return remote(region, region, self.hsend, self.hrecv, self.partner)

    def copy(self, k, phase, offset, source, target):
        region = weight_region(self.wo, k, self.core, source, WEIGHT_ORDER[k][:phase])
        return remote(
            region, region, self.wsend.at[k, phase, offset - 1], self.wrecv.at[k, phase, offset - 1],
            device_at(self.core, target),
        )

    def start(self, phase):
        for k in range(2):
            for offset in range(1, SIDE):
                target = shifted(self.spot, WEIGHT_ORDER[k][phase], offset)
                self.go(self.copy(k, phase, offset, self.spot, target))

    def forward_copy(self, k, phase, offset, core):
        source = shifted(self.spot, WEIGHT_ORDER[k][phase], -offset)
        region = weight_region(self.wo, k, core, source, WEIGHT_ORDER[k][:phase])
        return remote(
            region, region, self.fsend.at[k, phase, offset - 1], self.frecv.at[k, phase, offset - 1], self.partner
        )

    def arrive(self, phase):
        for k in range(2):
            for offset in range(1, SIDE):
                source = shifted(self.spot, WEIGHT_ORDER[k][phase], -offset)
                self.copy(k, phase, offset, source, self.spot).wait_recv()

    def forward(self, phase):
        for k in range(2):
            for offset in range(1, SIDE):
                self.go(self.forward_copy(k, phase, offset, self.core))

    def finish(self):
        self.line_forward(1 - self.core).wait_recv()
        for phase in range(2):
            for k in range(2):
                for offset in range(1, SIDE):
                    self.forward_copy(k, phase, offset, 1 - self.core).wait_recv()


def spread_heads(pairs):
    lane = lax.broadcasted_iota(jnp.int32, (8, 2 * HEAD_LANES), 1)
    low = lane < HEAD_LANES
    first, second = pairs[:8], pairs[8:]
    return jnp.concatenate(
        [
            jnp.where(low, first, 0.0),
            jnp.where(low, pltpu.roll(first, HEAD_LANES, 1), 0.0),
            jnp.where(low, 0.0, pltpu.roll(second, HEAD_LANES, 1)),
            jnp.where(low, 0.0, second),
        ],
        axis=0,
    )


def pair_heads(heads):
    lane = lax.broadcasted_iota(jnp.int32, (8, 2 * HEAD_LANES), 1)
    low = lane < HEAD_LANES
    first = jnp.where(low, heads[:8], pltpu.roll(heads[8:16], HEAD_LANES, 1))
    second = jnp.where(low, pltpu.roll(heads[16:24], HEAD_LANES, 1), heads[24:])
    return jnp.concatenate([first, second], axis=0)


def attend_some(first, count, lengths_ref, keys_ref, values_ref, gates_ref, pairs_ref, fresh_ref, gate_ref, mixed_ref):
    slots = keys_ref.shape[1]
    place = lax.broadcasted_iota(jnp.int32, (2, slots), 1)
    column = lax.broadcasted_iota(jnp.int32, (2, ROWS), 1)
    state = []
    for step in range(count):
        b = first + step
        queries = spread_heads(pairs_ref[b])
        scores = lax.dot_general(
            queries.astype(BF16), keys_ref[b], NT, preferred_element_type=F32
        )
        length = lengths_ref[b]
        sums = gates_ref[b]
        latest = jnp.sum(jnp.where(place == length - 1, sums, 0.0), axis=1, keepdims=True)
        fresh_gate = jnp.sum(jnp.where(column == b, gate_ref[...], 0.0), axis=1, keepdims=True)
        offsets = jnp.where(place < length, latest - sums + fresh_gate, -jnp.inf)
        wide = jnp.concatenate(
            [jnp.broadcast_to(offsets[:1], (16, slots)), jnp.broadcast_to(offsets[1:], (16, slots))], axis=0
        )
        scores = scores + wide
        fresh = fresh_ref[pl.ds(b, 1), :]
        own = jnp.sum(queries * fresh[:, : 2 * HEAD_LANES], axis=1, keepdims=True)
        state.append((scores, own, fresh[:, 2 * HEAD_LANES :]))
    for step, (scores, own, fresh_value) in enumerate(state):
        b = first + step
        highest = jnp.maximum(jnp.max(scores, axis=1, keepdims=True), own)
        past = jnp.exp(scores - highest)
        own = jnp.exp(own - highest)
        ratio = 1.0 / (jnp.sum(past, axis=1, keepdims=True) + own)
        weights = (past * ratio).astype(BF16)
        own_weight = (own * ratio).astype(BF16).astype(F32)
        mixed = jnp.dot(weights, values_ref[b], preferred_element_type=F32) + own_weight * fresh_value
        mixed_ref[b] = pair_heads(mixed)


def step_kernel(
    lengths_ref, tokens_hbm, keys_hbm, values_hbm, gates_hbm, query_hbm, key_hbm, value_hbm, forget_hbm, ow_hbm,
    routes_hbm, shares_hbm, gate_hbm, up_hbm, down_hbm, dgate_ref, dup_ref, ddown_ref,
    scale_ref, gain_ref, bias_ref, out_ref,
    tokens_ref, keys_ref, values_ref, gates_ref, wq_ref, wkv_ref, forget_ref, wo_ref, routes_ref, shares_ref,
    pairs_ref, mixed_ref, fresh_ref, newgate_ref, line_ref, sent_ref, back_ref, settled_ref,
    rows_ref, wg_ref, wu_ref, wd_ref, factor_ref, part_ref, twin_ref, r0_ref, r1_ref, r2_ref, s1_ref, s2_ref,
    wsem, asem, owsem, wxsend, wxrecv, wwsend, wwrecv, wfsend, wfrecv, whsend, whrecv,
    lsend, lrecv, bsend, brecv,
    gsend, grecv, fsend, frecv, osend, orecv, tsend, trecv, rsend, rrecv,
):
    core, spot = position()
    depth = WIDTH // GROUP
    small = [
        pltpu.make_async_copy(tokens_hbm, tokens_ref, asem.at[0]),
        pltpu.make_async_copy(forget_hbm, forget_ref, asem.at[1]),
        pltpu.make_async_copy(key_hbm, wkv_ref.at[:, pl.ds(0, 128)], asem.at[2]),
        pltpu.make_async_copy(value_hbm, wkv_ref.at[:, pl.ds(128, 128)], asem.at[3]),
    ]
    wide = [
        pltpu.make_async_copy(
            query_hbm.at[pl.ds(i * depth, depth)], wq_ref.at[pl.ds(i * depth, depth)], asem.at[4 + i]
        )
        for i in range(GROUP)
    ]
    cache = [
        pltpu.make_async_copy(keys_hbm, keys_ref, asem.at[8]),
        pltpu.make_async_copy(values_hbm, values_ref, asem.at[9]),
        pltpu.make_async_copy(gates_hbm, gates_ref, asem.at[10]),
    ]
    loads = [
        pltpu.make_async_copy(gate_hbm, wg_ref.at[pl.ds(0, FFE)], wsem.at[0]),
        pltpu.make_async_copy(up_hbm, wu_ref.at[pl.ds(0, FFE)], wsem.at[1]),
        pltpu.make_async_copy(down_hbm, wd_ref.at[pl.ds(0, FFE)], wsem.at[2]),
        pltpu.make_async_copy(routes_hbm, routes_ref, wsem.at[3]),
        pltpu.make_async_copy(shares_hbm, shares_ref, wsem.at[4]),
    ]
    for load in small + wide:
        load.start()
    entry_barrier(core, spot)
    weights = WeightGather(
        ow_hbm, wo_ref, core, spot, owsem, wwsend, wwrecv, wxsend, wxrecv, wfsend, wfrecv, whsend, whrecv
    )
    weights.line_start()
    for load in cache + loads:
        load.start()

    for load in small:
        load.wait()
    tokens = tokens_ref[...]
    fresh_ref[...] = jnp.dot(tokens, wkv_ref[...], preferred_element_type=F32).astype(BF16).astype(F32)
    raw = lax.dot_general(forget_ref[...], tokens, NT, preferred_element_type=F32)
    newgate_ref[...] = jnp.minimum(raw, 0.0) - jnp.log1p(jnp.exp(-jnp.abs(raw)))
    query = jnp.zeros((ROWS, WIDTH), F32)
    for i in range(GROUP):
        wide[i].wait()
        query = query + jnp.dot(
            tokens[:, i * depth : (i + 1) * depth], wq_ref[i * depth : (i + 1) * depth, :], preferred_element_type=F32
        )
    query = query.astype(BF16).astype(F32) * HEAD_LANES**-0.5
    flat = pairs_ref.reshape(ROWS * 16, 128)
    for i in range(16):
        flat[pl.ds(i, ROWS, stride=16), :] = query[:, 128 * i : 128 * (i + 1)]
    weights.line_arrive()
    weights.start(0)
    for load in cache:
        load.wait()

    def some(i, carry):
        attend_some(
            i * ATTEND, ATTEND, lengths_ref, keys_ref, values_ref, gates_ref, pairs_ref, fresh_ref, newgate_ref,
            mixed_ref,
        )
        return carry

    turns = ROWS // ATTEND
    lax.fori_loop(0, turns // 2, some, 0)
    weights.arrive(0)
    weights.start(1)
    weights.forward(0)
    lax.fori_loop(turns // 2, turns, some, 0)

    flat = mixed_ref.reshape(ROWS * 16, 128)
    attended = jnp.concatenate([flat[pl.ds(i, ROWS, stride=16), :] for i in range(16)], axis=1).astype(BF16)
    line_ref[spot[2]] = attended

    def line_copy(offset, source, target):
        return remote(
            line_ref.at[source[2]], line_ref.at[source[2]], lsend.at[offset - 1], lrecv.at[offset - 1],
            device_at(core, target),
        )

    for offset in range(1, SIDE):
        weights.go(line_copy(offset, spot, shifted(spot, 2, offset)))

    for load in loads:
        load.wait()
    pad = jnp.zeros((FFP - FFE - FFD, WIDTH), BF16)
    for ref, dense in ((wg_ref, dgate_ref[...]), (wu_ref, dup_ref[...])):
        ref[FFE:, :] = jnp.concatenate([dense, pad], axis=0)
    ddown = (ddown_ref[...].astype(F32) * scale_ref[...]).astype(BF16)
    wd_ref[FFE:, :] = jnp.concatenate([ddown, pad], axis=0)
    expert = lax.axis_index("ep") // (2 * SIDE * SIDE * SIDE // EXPERTS)
    picked = jnp.where(routes_ref[...] == expert, shares_ref[...], 0.0)
    factor = jnp.sum(picked, axis=0, keepdims=True)
    turned = jnp.transpose(jnp.broadcast_to(factor, (8, factor.shape[1])))
    factor_ref[...] = turned.reshape(factor_ref.shape)

    weights.arrive(1)
    weights.forward(1)
    for offset in range(1, SIDE):
        line_copy(offset, shifted(spot, 2, -offset), spot).wait_recv()
    weights.finish()
    lines = line_ref.reshape(SIDE * ROWS, WIDTH)[...]
    sent_ref.reshape(SIDE * ROWS, PROJ)[...] = jnp.dot(
        lines, wo_ref.reshape(WIDTH, PROJ)[...], preferred_element_type=F32
    )

    def back_copy(offset, source, target):
        return remote(
            sent_ref.at[target[2]], back_ref.at[source[2]], bsend.at[offset - 1], brecv.at[offset - 1],
            device_at(core, target),
        )

    for offset in range(1, SIDE):
        weights.go(back_copy(offset, spot, shifted(spot, 2, offset)))
    back_ref[spot[2]] = sent_ref[spot[2]]
    for offset in range(1, SIDE):
        back_copy(offset, shifted(spot, 2, -offset), spot).wait_recv()
    projected = jnp.concatenate([back_ref[i] for i in range(SIDE)], axis=1)
    settled = norm_rows(residual_scale * tokens.astype(F32) + projected, gain_ref[0:1, :], bias_ref[0:1, :])
    settled_ref[...] = settled
    rows_ref[(core,) + spot] = settled

    started = gather_rows(rows_ref, core, spot, gsend, grecv, fsend, frecv, osend, orecv)

    block = 2 * SIDE * SIDE * ROWS
    lane = lax.broadcasted_iota(jnp.int32, (1, FFP), 1)

    def part_of(half, plane):
        x = rows_ref.at[half, pl.ds(plane, 2)].reshape(block, WIDTH)[...]
        gate = lax.dot_general(x, wg_ref[...], NT, preferred_element_type=F32)
        up = lax.dot_general(x, wu_ref[...], NT, preferred_element_type=F32)
        weight = factor_ref[pl.ds(plane * SIDE * SIDE, 2 * SIDE * SIDE), half].reshape(block, 8)[:, :1]
        weight = jnp.where(lane < FFE, weight, 1.0)
        hidden = (gate * jax.nn.sigmoid(gate) * up * weight).astype(BF16)
        return jnp.dot(hidden, wd_ref[...], preferred_element_type=F32)

    partner = device_at(1 - core, spot)

    def twin_copy(i):
        return remote(
            part_ref.at[1 - core, pl.ds(2 * i, 2)], twin_ref.at[pl.ds(2 * i, 2)], tsend.at[i], trecv.at[i], partner
        )

    def far(i, carry):
        part_ref.at[1 - core, pl.ds(2 * i, 2)].reshape(block, WIDTH)[...] = part_of(1 - core, 2 * i).astype(BF16)
        twin_copy(i).start()
        return carry

    lax.fori_loop(0, SIDE // 2, far, 0)

    def near(i, carry):
        value = part_of(core, 2 * i)
        twin_copy(i).wait_recv()
        value = value + twin_ref.at[pl.ds(2 * i, 2)].reshape(block, WIDTH)[...].astype(F32)
        part_ref.at[core, pl.ds(2 * i, 2)].reshape(block, WIDTH)[...] = value.astype(BF16)
        return carry

    lax.fori_loop(0, SIDE // 2, near, 0)

    sums = ((part_ref, r0_ref, s1_ref), (s1_ref, r1_ref, s2_ref), (s2_ref, r2_ref, None))

    def slab(ref, phase, k, value):
        dims = left_over(k, phase)
        dim = GATHER_ORDER[k][::-1][phase]
        where = tuple(value if d == dim else pl.ds(0, SIDE) for d in dims)
        if phase == 0:
            where = (core,) + where
        return ref.at[where + (pl.ds(0, ROWS), columns(k))]

    def landed(ref, phase, k, index):
        where = (index,) + tuple(pl.ds(0, SIDE) for _ in range(2 - phase))
        return ref.at[where + (pl.ds(0, ROWS), columns(k))]

    def reduce_copy(phase, k, offset):
        dim = GATHER_ORDER[k][::-1][phase]
        target = shifted(spot, dim, offset)
        return remote(
            slab(sums[phase][0], phase, k, target[dim]), landed(sums[phase][1], phase, k, offset - 1),
            rsend.at[k, phase, offset - 1], rrecv.at[k, phase, offset - 1], device_at(core, target),
        )

    def reduce_start(phase, k):
        for offset in range(1, SIDE):
            copy = reduce_copy(phase, k, offset)
            copy.start()
            started.append(copy)

    def reduce_sum(phase, k):
        dim = GATHER_ORDER[k][::-1][phase]
        total = slab(sums[phase][0], phase, k, spot[dim])[...].astype(F32)
        for offset in range(1, SIDE):
            reduce_copy(phase, k, offset).wait_recv()
            total = total + landed(sums[phase][1], phase, k, offset - 1)[...].astype(F32)
        return total

    for k in range(3):
        reduce_start(0, k)
    for phase in range(2):
        for k in range(3):
            where = tuple(pl.ds(0, SIDE) for _ in range(2 - phase)) + (pl.ds(0, ROWS), columns(k))
            sums[phase][2][where] = reduce_sum(phase, k).astype(BF16)
            reduce_start(phase + 1, k)
    ffn = jnp.concatenate([reduce_sum(2, k) for k in range(3)], axis=-1)
    out_ref[...] = norm_rows(
        residual_scale * settled_ref[...].astype(F32) + ffn, gain_ref[1:2, :], bias_ref[1:2, :]
    )
    for copy in weights.started + started:
        copy.wait_send()
    for i in range(SIDE // 2):
        twin_copy(i).wait_send()


def step_call(lengths, *operands):
    vmem = pl.BlockSpec(memory_space=pltpu.VMEM)
    hbm = pl.BlockSpec(memory_space=pltpu.HBM)
    sem = pltpu.SemaphoreType.DMA
    cube = (SIDE, SIDE, SIDE, ROWS, WIDTH)
    slots = operands[1].shape[1]
    peers = SIDE - 1
    return pl.pallas_call(
        step_kernel,
        out_shape=jax.ShapeDtypeStruct((ROWS, WIDTH), BF16),
        in_specs=[pl.BlockSpec(memory_space=pltpu.SMEM)] + [hbm] * 14 + [vmem] * 6,
        out_specs=vmem,
        scratch_shapes=[
            pltpu.VMEM((ROWS, WIDTH), BF16),
            pltpu.VMEM((ROWS, slots, 128), BF16),
            pltpu.VMEM((ROWS, slots, 128), BF16),
            pltpu.VMEM((ROWS, 2, slots), F32),
            pltpu.VMEM((WIDTH, WIDTH), BF16),
            pltpu.VMEM((WIDTH, 256), BF16),
            pltpu.VMEM((2, WIDTH), BF16),
            pltpu.VMEM((SIDE, SIDE, SIDE, 2, 2 * ROWS, PROJ), BF16),
            pltpu.VMEM((2, 2 * SIDE**3 * ROWS), jnp.int32),
            pltpu.VMEM((2, 2 * SIDE**3 * ROWS), F32),
            pltpu.VMEM((ROWS, 16, 128), F32),
            pltpu.VMEM((ROWS, 16, 128), F32),
            pltpu.VMEM((ROWS, 256), F32),
            pltpu.VMEM((2, ROWS), F32),
            pltpu.VMEM((SIDE, ROWS, WIDTH), BF16),
            pltpu.VMEM((SIDE, ROWS, PROJ), F32),
            pltpu.VMEM((SIDE, ROWS, PROJ), F32),
            pltpu.VMEM((ROWS, WIDTH), BF16),
            pltpu.VMEM((2,) + cube, BF16),
            pltpu.VMEM((FFP, WIDTH), BF16),
            pltpu.VMEM((FFP, WIDTH), BF16),
            pltpu.VMEM((FFP, WIDTH), BF16),
            pltpu.VMEM((SIDE**3, 2, ROWS, 8), F32),
            pltpu.VMEM((2,) + cube, BF16),
            pltpu.VMEM(cube, BF16),
            pltpu.VMEM((peers,) + cube[1:], BF16),
            pltpu.VMEM((peers,) + cube[2:], BF16),
            pltpu.VMEM((peers,) + cube[3:], BF16),
            pltpu.VMEM(cube[1:], BF16),
            pltpu.VMEM(cube[2:], BF16),
            sem((5,)), sem((11,)), sem,
            sem((peers,)), sem((peers,)),
            sem((2, 2, peers)), sem((2, 2, peers)),
            sem((2, 2, peers)), sem((2, 2, peers)),
            sem, sem,
            sem((peers,)), sem((peers,)), sem((peers,)), sem((peers,)),
            sem((3, 3, peers)), sem((3, 3, peers)),
            sem((3, 3, peers)), sem((3, 3, peers)),
            sem, sem,
            sem((SIDE // 2,)), sem((SIDE // 2,)),
            sem((3, 3, peers)), sem((3, 3, peers)),
        ],
        compiler_params=pltpu.CompilerParams(
            collective_id=0, has_side_effects=True, vmem_limit_bytes=60 * 2**20
        ),
        name="step",
    )(lengths, *operands)


def local(
    tokens,
    cache_keys,
    cache_values,
    cum_gates,
    lengths,
    query_weight,
    key_weight,
    value_weight,
    forget_weight,
    out_weight,
    norm_gain,
    norm_bias,
    dense_gate_weight,
    dense_up_weight,
    dense_down_weight,
    dense_scale,
    expert_gate_weight,
    expert_up_weight,
    expert_down_weight,
    routes,
    route_weights,
):
    return step_call(
        lengths,
        tokens,
        cache_keys,
        cache_values,
        jnp.transpose(cum_gates, (0, 2, 1)),
        query_weight,
        key_weight,
        value_weight,
        jnp.transpose(forget_weight),
        out_weight,
        jnp.transpose(routes),
        jnp.transpose(route_weights),
        jnp.transpose(expert_gate_weight),
        jnp.transpose(expert_up_weight),
        expert_down_weight,
        jnp.transpose(dense_gate_weight),
        jnp.transpose(dense_up_weight),
        dense_down_weight,
        dense_scale.reshape(1, -1),
        norm_gain,
        norm_bias,
    )


def solution(mesh):
    return jax.shard_map(
        local,
        mesh=mesh,
        in_specs=(
            P("ep", None),
            P("ep", None, None),
            P("ep", None, None),
            P("ep", None, None),
            P("ep"),
            P(),
            P(),
            P(),
            P(),
            P("ep", None),
            P(),
            P(),
            P(None, "ep"),
            P(None, "ep"),
            P("ep", None),
            P(),
            P(None, "ep"),
            P(None, "ep"),
            P("ep", None),
            P(),
            P(),
        ),
        out_specs=P("ep", None),
        check_vma=False,
    )
```

```python
import functools

import jax
import jax.numpy as jnp
from jax import lax
from jax.experimental import pallas as pl
from jax.experimental.pallas import tpu as pltpu
from jax.sharding import PartitionSpec as P

MESH = pl.DeviceIdType.MESH
F32 = jnp.float32
BF16 = jnp.bfloat16
SIDE = 4
ROWS = 8
WIDTH = 2048
EXPERTS = 8
FFE = 448
FFD = 44
FFP = 512
CHUNKS = ((0, 768), (768, 640), (1408, 640))
GATHER_ORDER = ((2, 1, 0), (0, 2, 1), (1, 0, 2))
ATTEND = 4
residual_scale = 1.4142135
norm_eps = 1e-05


def norm_rows(values, gain_row, shift_row):
    centre = jnp.mean(values, axis=-1, keepdims=True)
    centred = values - centre
    spread = jnp.mean(centred * centred, axis=-1, keepdims=True)
    return (centred * lax.rsqrt(spread + norm_eps) * gain_row + shift_row).astype(BF16)


def position():
    me = lax.axis_index("ep")
    core = me % 2
    x = (me // 2) % SIDE
    y = (me // (2 * SIDE)) % SIDE
    z = me // (2 * SIDE * SIDE)
    return core, (z, y, x)


def device_at(core, spot):
    z, y, x = spot
    return (((z * SIDE + y) * SIDE + x) * 2 + core,)


def moved(spot, dim, value):
    return tuple(value if d == dim else spot[d] for d in range(3))


def shifted(spot, dim, offset):
    return moved(spot, dim, (spot[dim] + offset + SIDE) % SIDE)


def columns(k):
    return pl.ds(CHUNKS[k][0], CHUNKS[k][1])


def remote(src, dst, send, recv, target):
    return pltpu.make_async_remote_copy(
        src_ref=src, dst_ref=dst, send_sem=send, recv_sem=recv, device_id=target, device_id_type=MESH
    )


def entry_signal(core, spot):
    barrier = pltpu.get_barrier_semaphore()
    for offset in range(SIDE):
        pl.semaphore_signal(
            barrier, inc=1, device_id=device_at(1 - core, shifted(spot, 2, offset)), device_id_type=MESH
        )
    for dim in range(3):
        for offset in range(1, SIDE):
            pl.semaphore_signal(
                barrier, inc=1, device_id=device_at(core, shifted(spot, dim, offset)), device_id_type=MESH
            )


def entry_wait():
    pl.semaphore_wait(pltpu.get_barrier_semaphore(), 3 * (SIDE - 1) + SIDE)


PROJ = 256
HALF = 128
WEIGHT_ORDER = ((1, 0), (0, 1))
NT = (((1,), (1,)), ((), ()))
GROUP = 4
HEAD_LANES = 64
PEERS = SIDE - 1
PIECES = (1, 3, 2)
LINE = tuple((offset, flip) for offset in range(SIDE) for flip in range(2))[1:]


def spread_heads(pairs):
    lane = lax.broadcasted_iota(jnp.int32, (8, 2 * HEAD_LANES), 1)
    low = lane < HEAD_LANES
    first, second = pairs[:8], pairs[8:]
    return jnp.concatenate(
        [
            jnp.where(low, first, 0.0),
            jnp.where(low, pltpu.roll(first, HEAD_LANES, 1), 0.0),
            jnp.where(low, 0.0, pltpu.roll(second, HEAD_LANES, 1)),
            jnp.where(low, 0.0, second),
        ],
        axis=0,
    )


def pair_heads(heads):
    lane = lax.broadcasted_iota(jnp.int32, (8, 2 * HEAD_LANES), 1)
    low = lane < HEAD_LANES
    first = jnp.where(low, heads[:8], pltpu.roll(heads[8:16], HEAD_LANES, 1))
    second = jnp.where(low, pltpu.roll(heads[16:24], HEAD_LANES, 1), heads[24:])
    return jnp.concatenate([first, second], axis=0)


def attend_some(first, count, lengths_ref, keys_ref, values_ref, gates_ref, pairs_ref, fresh_ref, gate_ref, mixed_ref):
    slots = keys_ref.shape[1]
    place = lax.broadcasted_iota(jnp.int32, (2, slots), 1)
    column = lax.broadcasted_iota(jnp.int32, (2, ROWS), 1)
    state = []
    for step in range(count):
        b = first + step
        queries = spread_heads(pairs_ref[b])
        scores = lax.dot_general(
            queries.astype(BF16), keys_ref[b], NT, preferred_element_type=F32
        )
        length = lengths_ref[b]
        sums = gates_ref[b]
        latest = jnp.sum(jnp.where(place == length - 1, sums, 0.0), axis=1, keepdims=True)
        fresh_gate = jnp.sum(jnp.where(column == b, gate_ref[...], 0.0), axis=1, keepdims=True)
        offsets = jnp.where(place < length, latest - sums + fresh_gate, -jnp.inf)
        wide = jnp.concatenate(
            [jnp.broadcast_to(offsets[:1], (16, slots)), jnp.broadcast_to(offsets[1:], (16, slots))], axis=0
        )
        scores = scores + wide
        fresh = fresh_ref[pl.ds(b, 1), :]
        own = jnp.sum(queries * fresh[:, : 2 * HEAD_LANES], axis=1, keepdims=True)
        state.append((scores, own, fresh[:, 2 * HEAD_LANES :]))
    for step, (scores, own, fresh_value) in enumerate(state):
        b = first + step
        highest = jnp.maximum(jnp.max(scores, axis=1, keepdims=True), own)
        past = jnp.exp(scores - highest)
        own = jnp.exp(own - highest)
        ratio = 1.0 / (jnp.sum(past, axis=1, keepdims=True) + own)
        weights = (past * ratio).astype(BF16)
        own_weight = (own * ratio).astype(BF16).astype(F32)
        mixed = jnp.dot(weights, values_ref[b], preferred_element_type=F32) + own_weight * fresh_value
        mixed_ref[b] = pair_heads(mixed)


class Transfers:
    def __init__(self):
        self.started = []

    def go(self, copy):
        copy.start()
        self.started.append(copy)

    def drain(self):
        for copy in self.started:
            copy.wait_send()


class Spread:
    def __init__(self, moves, view, core, spot, first, second, send1, recv1, send2, recv2):
        self.moves, self.view, self.core, self.spot = moves, view, core, spot
        self.first, self.second = first, second
        self.send1, self.recv1, self.send2, self.recv2 = send1, recv1, send2, recv2

    def near_copy(self, offset, source, target):
        region = self.view(source)
        return remote(region, region, self.send1.at[offset - 1], self.recv1.at[offset - 1], device_at(self.core, target))

    def far_copy(self, offset, piece, source, target):
        region = self.view(shifted(source, self.first, -piece))
        return remote(
            region, region, self.send2.at[offset - 1, piece], self.recv2.at[offset - 1, piece],
            device_at(self.core, target),
        )

    def far_start(self, piece):
        for offset in PIECES:
            self.moves.go(self.far_copy(offset, piece, self.spot, shifted(self.spot, self.second, offset)))

    def start(self):
        for offset in PIECES:
            self.moves.go(self.near_copy(offset, self.spot, shifted(self.spot, self.first, offset)))
        self.far_start(0)

    def relay(self, offset):
        self.near_copy(offset, shifted(self.spot, self.first, -offset), self.spot).wait_recv()
        self.far_start(offset)

    def far_arrive(self, offset):
        source = shifted(self.spot, self.second, -offset)
        for piece in range(SIDE):
            self.far_copy(offset, piece, source, self.spot).wait_recv()


def step_kernel(
    lengths_hbm, tokens_hbm, keys_hbm, values_hbm, gates_hbm, query_hbm, key_hbm, value_hbm, forget_hbm, ow_hbm,
    routes_hbm, shares_hbm, gate_hbm, up_hbm, down_hbm, dgate_hbm, dup_hbm, ddown_hbm,
    scale_hbm, gain_hbm, bias_hbm, out_ref,
    lengths_ref, tokens_ref, keys_ref, values_ref, gates_ref, wq_ref, wkv_ref, forget_ref, ow_ref, wo_ref,
    routes_ref, shares_ref, scale_ref, gain_ref, bias_ref,
    pairs_ref, mixed_ref, fresh_ref, newgate_ref, line_ref, sent_ref, back_ref, settled_ref,
    rows_ref, wg_ref, wu_ref, wd_ref, dense_ref, factor_ref, part_ref, r0_ref, r1_ref, r2_ref, s1_ref, s2_ref,
    asem, wsem, swsend, swrecv, xsend, xrecv, w1send, w1recv, w2send, w2recv,
    lsend, lrecv, bsend, brecv,
    g0send, g0recv, g1send, g1recv, g2send, g2recv,
    rsend, rrecv, r1send, r1recv, r2send, r2recv,
):
    core, spot = position()
    partner = device_at(1 - core, spot)
    entry_signal(core, spot)
    depth = WIDTH // GROUP
    first_loads = [(ow_hbm, ow_ref)]
    small = [
        (tokens_hbm, tokens_ref),
        (forget_hbm, forget_ref),
        (key_hbm, wkv_ref.at[:, pl.ds(0, 128)]),
        (value_hbm, wkv_ref.at[:, pl.ds(128, 128)]),
    ]
    wide = [(query_hbm.at[pl.ds(i * depth, depth)], wq_ref.at[pl.ds(i * depth, depth)]) for i in range(GROUP)]
    cache = [
        (keys_hbm, keys_ref), (values_hbm, values_ref), (gates_hbm, gates_ref), (lengths_hbm, lengths_ref),
        (gain_hbm, gain_ref), (bias_hbm, bias_ref), (scale_hbm, scale_ref),
        (routes_hbm, routes_ref), (shares_hbm, shares_ref),
    ]
    tables = ((gate_hbm, wg_ref), (up_hbm, wu_ref), (down_hbm, wd_ref))
    dense = (dgate_hbm, dup_hbm, ddown_hbm)
    shard = [(hbm, ref.at[core, pl.ds(0, FFE)]) for hbm, ref in tables]
    shard += [(hbm, dense_ref.at[core, i]) for i, hbm in enumerate(dense)]
    count = 0
    groups = []
    for group in (first_loads, small, wide, cache, shard):
        copies = []
        for source, target in group:
            copies.append(pltpu.make_async_copy(source, target, asem.at[count]))
            count += 1
        groups.append(copies)
    first_loads, small, wide, cache, shard = groups
    for load in first_loads + small + wide + cache:
        load.start()

    moves = Transfers()
    me = spot[2] * 2 + core

    def swap_copy(table, part, owner):
        hbm, ref = tables[table]
        size = FFE // 4
        here = pl.ds(part * size, size)
        return remote(
            hbm.at[here], ref.at[owner, here], swsend.at[table * 4 + part], swrecv.at[table * 4 + part], partner
        )

    def swap_dense(i, owner):
        return remote(dense[i], dense_ref.at[owner, i], swsend.at[12 + i], swrecv.at[12 + i], partner)

    def swap_start(table):
        for part in range(4):
            moves.go(swap_copy(table, part, core))
        moves.go(swap_dense(table, core))

    def line_target(offset, flip, sign=1):
        return (core if flip == 0 else 1 - core), shifted(spot, 2, sign * offset)

    def block_copy(index, from_core, source, to_core, target):
        z, y, x = source
        here = pl.multiple_of((target[2] * 2 + to_core) * PROJ, PROJ)
        return remote(
            ow_ref.at[:, pl.ds(here, PROJ)], wo_ref.at[z, y, x, from_core], xsend.at[index], xrecv.at[index],
            device_at(to_core, target),
        )

    for load in first_loads:
        load.wait()
    wo_ref[spot[0], spot[1], spot[2], core] = ow_ref[:, pl.ds(pl.multiple_of(me * PROJ, PROJ), PROJ)]
    entry_wait()
    for index, (offset, flip) in enumerate(LINE):
        moves.go(block_copy(index, core, spot, *line_target(offset, flip)))
    for load in shard:
        load.start()

    def weight_view(k):
        def view(source):
            return wo_ref.at[
                source[0], source[1], pl.ds(0, SIDE), pl.ds(0, 2), pl.ds(0, 2 * ROWS), pl.ds(k * HALF, HALF)
            ]

        return view

    weights = [
        Spread(
            moves, weight_view(k), core, spot, *WEIGHT_ORDER[k],
            w1send.at[k], w1recv.at[k], w2send.at[k], w2recv.at[k],
        )
        for k in range(2)
    ]

    for load in small:
        load.wait()
    tokens = tokens_ref[...]
    fresh_ref[...] = jnp.dot(tokens, wkv_ref[...], preferred_element_type=F32).astype(BF16).astype(F32)
    raw = lax.dot_general(forget_ref[...], tokens, NT, preferred_element_type=F32)
    newgate_ref[...] = jnp.minimum(raw, 0.0) - jnp.log1p(jnp.exp(-jnp.abs(raw)))
    query = jnp.zeros((ROWS, WIDTH), F32)
    for i in range(GROUP):
        wide[i].wait()
        query = query + jnp.dot(
            tokens[:, i * depth : (i + 1) * depth], wq_ref[i * depth : (i + 1) * depth, :], preferred_element_type=F32
        )
    query = query.astype(BF16).astype(F32) * HEAD_LANES**-0.5
    flat = pairs_ref.reshape(ROWS * 16, 128)
    for i in range(16):
        flat[pl.ds(i, ROWS, stride=16), :] = query[:, 128 * i : 128 * (i + 1)]
    for index, (offset, flip) in enumerate(LINE):
        from_core, source = line_target(offset, flip, -1)
        block_copy(index, from_core, source, core, spot).wait_recv()
    for weight in weights:
        weight.start()
    swap_start(0)
    for load in cache:
        load.wait()

    def some(i, carry):
        attend_some(
            i * ATTEND, ATTEND, lengths_ref, keys_ref, values_ref, gates_ref, pairs_ref, fresh_ref, newgate_ref,
            mixed_ref,
        )
        return carry

    lax.fori_loop(0, ROWS // ATTEND, some, 0)
    flat = mixed_ref.reshape(ROWS * 16, 128)
    attended = jnp.concatenate([flat[pl.ds(i, ROWS, stride=16), :] for i in range(16)], axis=1).astype(BF16)
    line_ref[spot[2], core] = attended

    def line_copy(index, from_core, source, to_core, target):
        here = line_ref.at[source[2], from_core]
        return remote(here, here, lsend.at[index], lrecv.at[index], device_at(to_core, target))

    for index, (offset, flip) in enumerate(LINE):
        moves.go(line_copy(index, core, spot, *line_target(offset, flip)))
    for offset in PIECES:
        for weight in weights:
            weight.relay(offset)
    swap_start(1)
    swap_start(2)

    expert = lax.axis_index("ep") // (2 * SIDE * SIDE * SIDE // EXPERTS)
    picked = jnp.where(routes_ref[...] == expert, shares_ref[...], 0.0)
    factor = jnp.sum(picked, axis=0, keepdims=True)
    turned = jnp.transpose(jnp.broadcast_to(factor, (8, factor.shape[1])))
    factor_ref[...] = turned.reshape(factor_ref.shape)

    for index, (offset, flip) in enumerate(LINE):
        from_core, source = line_target(offset, flip, -1)
        line_copy(index, from_core, source, core, spot).wait_recv()
    for offset in PIECES:
        for weight in weights:
            weight.far_arrive(offset)
    lines = line_ref.reshape(2 * SIDE * ROWS, WIDTH)[...]
    sent_ref.reshape(2 * SIDE * ROWS, PROJ)[...] = jnp.dot(
        lines, wo_ref.reshape(WIDTH, PROJ)[...], preferred_element_type=F32
    )

    def back_copy(index, from_core, source, to_core, target):
        return remote(
            sent_ref.at[target[2], to_core], back_ref.at[source[2], from_core], bsend.at[index], brecv.at[index],
            device_at(to_core, target),
        )

    for index, (offset, flip) in enumerate(LINE):
        moves.go(back_copy(index, core, spot, *line_target(offset, flip)))
    back_ref[spot[2], core] = sent_ref[spot[2], core]
    for index, (offset, flip) in enumerate(LINE):
        from_core, source = line_target(offset, flip, -1)
        back_copy(index, from_core, source, core, spot).wait_recv()
    projected = jnp.concatenate([back_ref[i // 2, i % 2] for i in range(2 * SIDE)], axis=1)
    settled = norm_rows(residual_scale * tokens.astype(F32) + projected, gain_ref[0:1, :], bias_ref[0:1, :])
    settled_ref[...] = settled
    rows_ref[spot] = settled

    def row_view(k):
        gone = GATHER_ORDER[k][0]

        def view(source):
            where = tuple(pl.ds(0, SIDE) if d == gone else source[d] for d in range(3))
            return rows_ref.at[where + (pl.ds(0, ROWS), columns(k))]

        return view

    def first_copy(k, offset, source, target):
        region = rows_ref.at[source + (pl.ds(0, ROWS), columns(k))]
        return remote(region, region, g0send.at[k, offset - 1], g0recv.at[k, offset - 1], device_at(core, target))

    for offset in PIECES:
        for k in range(3):
            moves.go(first_copy(k, offset, spot, shifted(spot, GATHER_ORDER[k][0], offset)))

    pad = jnp.zeros((FFP - FFE - FFD, WIDTH), BF16)

    def dense_rows(slot):
        for i, ref in ((0, wg_ref), (1, wu_ref), (2, wd_ref)):
            value = dense_ref[slot, i]
            if i == 2:
                value = (value.astype(F32) * scale_ref[...]).astype(BF16)
            ref[slot, FFE:, :] = jnp.concatenate([value, pad], axis=0)

    for load in shard:
        load.wait()
    dense_rows(core)
    spreads = [
        Spread(
            moves, row_view(k), core, spot, *GATHER_ORDER[k][1:],
            g1send.at[k], g1recv.at[k], g2send.at[k], g2recv.at[k],
        )
        for k in range(3)
    ]
    for k in range(3):
        for offset in PIECES:
            first_copy(k, offset, shifted(spot, GATHER_ORDER[k][0], -offset), spot).wait_recv()
        spreads[k].start()
    for offset in PIECES:
        for k in range(3):
            spreads[k].relay(offset)
    for table in range(3):
        for part in range(4):
            swap_copy(table, part, 1 - core).wait_recv()
        swap_dense(table, 1 - core).wait_recv()
    dense_rows(1 - core)
    for offset in PIECES:
        for k in range(3):
            spreads[k].far_arrive(offset)

    block = 2 * SIDE * SIDE * ROWS
    lane = lax.broadcasted_iota(jnp.int32, (1, 2 * FFP), 1) % FFP

    def ffn(i, carry):
        x = rows_ref.at[pl.ds(2 * i, 2)].reshape(block, WIDTH)[...]
        gate = lax.dot_general(x, wg_ref.reshape(2 * FFP, WIDTH)[...], NT, preferred_element_type=F32)
        up = lax.dot_general(x, wu_ref.reshape(2 * FFP, WIDTH)[...], NT, preferred_element_type=F32)
        weight = factor_ref[pl.ds(2 * i * SIDE * SIDE, 2 * SIDE * SIDE), core].reshape(block, 8)[:, :1]
        weight = jnp.where(lane < FFE, weight, 1.0)
        hidden = (gate * jax.nn.sigmoid(gate) * up * weight).astype(BF16)
        value = jnp.dot(hidden, wd_ref.reshape(2 * FFP, WIDTH)[...], preferred_element_type=F32)
        part_ref.at[pl.ds(2 * i, 2)].reshape(block, WIDTH)[...] = value.astype(BF16)
        return carry

    lax.fori_loop(0, SIDE // 2, ffn, 0)

    def dims_of(k):
        return GATHER_ORDER[k][::-1]

    def cell(ref, lead, k, phase, fixed):
        gone = dims_of(k)[:phase]
        where = tuple(fixed.get(d, pl.ds(0, SIDE)) for d in range(3) if d not in gone)
        return ref.at[lead + where + (pl.ds(0, ROWS), columns(k))]

    def send0(k, offset, piece, target):
        a, b, _ = dims_of(k)
        line = (spot[b] + piece) % SIDE
        return remote(
            cell(part_ref, (), k, 0, {a: target[a], b: line}), cell(r0_ref, (offset - 1,), k, 1, {b: line}),
            rsend.at[k, offset - 1, piece], rrecv.at[k, offset - 1, piece], device_at(core, target),
        )

    def send1(k, offset, target):
        b = dims_of(k)[1]
        return remote(
            cell(s1_ref, (), k, 1, {b: target[b]}), cell(r1_ref, (offset - 1,), k, 2, {}),
            r1send.at[k, offset - 1], r1recv.at[k, offset - 1], device_at(core, target),
        )

    def send2(k, offset, target):
        c = dims_of(k)[2]
        return remote(
            cell(s2_ref, (), k, 2, {c: target[c]}), cell(r2_ref, (offset - 1,), k, 3, {}),
            r2send.at[k, offset - 1], r2recv.at[k, offset - 1], device_at(core, target),
        )

    order = (2, 1, 3, 0)
    for piece in order:
        for offset in PIECES:
            for k in range(3):
                moves.go(send0(k, offset, piece, shifted(spot, dims_of(k)[0], offset)))
    for piece in order:
        for k in range(3):
            a, b, _ = dims_of(k)
            line = (spot[b] + piece) % SIDE
            total = cell(part_ref, (), k, 0, {a: spot[a], b: line})[...].astype(F32)
            for offset in PIECES:
                send0(k, offset, piece, spot).wait_recv()
                total = total + cell(r0_ref, (offset - 1,), k, 1, {b: line})[...].astype(F32)
            cell(s1_ref, (), k, 1, {b: line})[...] = total.astype(BF16)
            if piece:
                moves.go(send1(k, piece, shifted(spot, b, piece)))
    for k in range(3):
        b, c = dims_of(k)[1:]
        total = cell(s1_ref, (), k, 1, {b: spot[b]})[...].astype(F32)
        for offset in PIECES:
            send1(k, offset, spot).wait_recv()
            total = total + cell(r1_ref, (offset - 1,), k, 2, {})[...].astype(F32)
        cell(s2_ref, (), k, 2, {})[...] = total.astype(BF16)
        for offset in PIECES:
            moves.go(send2(k, offset, shifted(spot, c, offset)))
    sums = []
    for k in range(3):
        c = dims_of(k)[2]
        total = cell(s2_ref, (), k, 2, {c: spot[c]})[...].astype(F32)
        for offset in PIECES:
            send2(k, offset, spot).wait_recv()
            total = total + cell(r2_ref, (offset - 1,), k, 3, {})[...].astype(F32)
        sums.append(total)
    ffn_sum = jnp.concatenate(sums, axis=-1)
    out_ref[...] = norm_rows(
        residual_scale * settled_ref[...].astype(F32) + ffn_sum, gain_ref[1:2, :], bias_ref[1:2, :]
    )
    moves.drain()


def step_call(*operands):
    vmem = pl.BlockSpec(memory_space=pltpu.VMEM)
    hbm = pl.BlockSpec(memory_space=pltpu.HBM)
    sem = pltpu.SemaphoreType.DMA
    cube = (SIDE, SIDE, SIDE, ROWS, WIDTH)
    slots = operands[2].shape[1]
    line = len(LINE)
    return pl.pallas_call(
        step_kernel,
        out_shape=jax.ShapeDtypeStruct((ROWS, WIDTH), BF16),
        in_specs=[hbm] * len(operands),
        out_specs=vmem,
        scratch_shapes=[
            pltpu.SMEM((ROWS,), jnp.int32),
            pltpu.VMEM((ROWS, WIDTH), BF16),
            pltpu.VMEM((ROWS, slots, 128), BF16),
            pltpu.VMEM((ROWS, slots, 128), BF16),
            pltpu.VMEM((ROWS, 2, slots), F32),
            pltpu.VMEM((WIDTH, WIDTH), BF16),
            pltpu.VMEM((WIDTH, 256), BF16),
            pltpu.VMEM((2, WIDTH), BF16),
            pltpu.VMEM((2 * ROWS, WIDTH), BF16),
            pltpu.VMEM((SIDE, SIDE, SIDE, 2, 2 * ROWS, PROJ), BF16),
            pltpu.VMEM((2, 2 * SIDE**3 * ROWS), jnp.int32),
            pltpu.VMEM((2, 2 * SIDE**3 * ROWS), F32),
            pltpu.VMEM((1, WIDTH), F32),
            pltpu.VMEM((2, WIDTH), F32),
            pltpu.VMEM((2, WIDTH), F32),
            pltpu.VMEM((ROWS, 16, 128), F32),
            pltpu.VMEM((ROWS, 16, 128), F32),
            pltpu.VMEM((ROWS, 256), F32),
            pltpu.VMEM((2, ROWS), F32),
            pltpu.VMEM((SIDE, 2, ROWS, WIDTH), BF16),
            pltpu.VMEM((SIDE, 2, ROWS, PROJ), F32),
            pltpu.VMEM((SIDE, 2, ROWS, PROJ), F32),
            pltpu.VMEM((ROWS, WIDTH), BF16),
            pltpu.VMEM(cube, BF16),
            pltpu.VMEM((2, FFP, WIDTH), BF16),
            pltpu.VMEM((2, FFP, WIDTH), BF16),
            pltpu.VMEM((2, FFP, WIDTH), BF16),
            pltpu.VMEM((2, 3, FFD, WIDTH), BF16),
            pltpu.VMEM((SIDE**3, 2, ROWS, 8), F32),
            pltpu.VMEM(cube, BF16),
            pltpu.VMEM((PEERS,) + cube[1:], BF16),
            pltpu.VMEM((PEERS,) + cube[2:], BF16),
            pltpu.VMEM((PEERS,) + cube[3:], BF16),
            pltpu.VMEM(cube[1:], BF16),
            pltpu.VMEM(cube[2:], BF16),
            sem((24,)), sem((1,)), sem((15,)), sem((15,)),
            sem((line,)), sem((line,)),
            sem((2, PEERS)), sem((2, PEERS)), sem((2, PEERS, SIDE)), sem((2, PEERS, SIDE)),
            sem((line,)), sem((line,)), sem((line,)), sem((line,)),
            sem((3, PEERS)), sem((3, PEERS)),
            sem((3, PEERS)), sem((3, PEERS)), sem((3, PEERS, SIDE)), sem((3, PEERS, SIDE)),
            sem((3, PEERS, SIDE)), sem((3, PEERS, SIDE)),
            sem((3, PEERS)), sem((3, PEERS)), sem((3, PEERS)), sem((3, PEERS)),
        ],
        compiler_params=pltpu.CompilerParams(
            collective_id=0, has_side_effects=True, vmem_limit_bytes=60 * 2**20
        ),
        name="step",
    )(*operands)


def local(
    tokens,
    cache_keys,
    cache_values,
    cum_gates,
    lengths,
    query_weight,
    key_weight,
    value_weight,
    forget_weight,
    out_weight,
    norm_gain,
    norm_bias,
    dense_gate_weight,
    dense_up_weight,
    dense_down_weight,
    dense_scale,
    expert_gate_weight,
    expert_up_weight,
    expert_down_weight,
    routes,
    route_weights,
):
    return step_call(
        lengths,
        tokens,
        cache_keys,
        cache_values,
        jnp.transpose(cum_gates, (0, 2, 1)),
        query_weight,
        key_weight,
        value_weight,
        jnp.transpose(forget_weight),
        out_weight,
        jnp.transpose(routes),
        jnp.transpose(route_weights),
        jnp.transpose(expert_gate_weight),
        jnp.transpose(expert_up_weight),
        expert_down_weight,
        jnp.transpose(dense_gate_weight),
        jnp.transpose(dense_up_weight),
        dense_down_weight,
        dense_scale.reshape(1, -1),
        norm_gain,
        norm_bias,
    )


def solution(mesh):
    return jax.shard_map(
        local,
        mesh=mesh,
        in_specs=(
            P("ep", None),
            P("ep", None, None),
            P("ep", None, None),
            P("ep", None, None),
            P("ep"),
            P(),
            P(),
            P(),
            P(),
            P("ep", None),
            P(),
            P(),
            P(None, "ep"),
            P(None, "ep"),
            P("ep", None),
            P(),
            P(None, "ep"),
            P(None, "ep"),
            P("ep", None),
            P(),
            P(),
        ),
        out_specs=P("ep", None),
        check_vma=False,
    )
```

```python
import functools

import jax
import jax.numpy as jnp
from jax import lax
from jax.experimental import pallas as pl
from jax.experimental.pallas import tpu as pltpu
from jax.sharding import PartitionSpec as P

MESH = pl.DeviceIdType.MESH
F32 = jnp.float32
BF16 = jnp.bfloat16
SIDE = 4
ROWS = 8
WIDTH = 2048
EXPERTS = 8
FFE = 448
FFD = 44
FFP = 512
CHUNKS = ((0, 768), (768, 640), (1408, 640))
REDUCE_CHUNKS = ((0, 768), (768, 512), (1280, 768))
GATHER_ORDER = ((2, 1, 0), (0, 2, 1), (1, 0, 2))
ATTEND = 4
residual_scale = 1.4142135
norm_eps = 1e-05


def norm_rows(values, gain_row, shift_row):
    centre = jnp.mean(values, axis=-1, keepdims=True)
    centred = values - centre
    spread = jnp.mean(centred * centred, axis=-1, keepdims=True)
    return (centred * lax.rsqrt(spread + norm_eps) * gain_row + shift_row).astype(BF16)


def position():
    me = lax.axis_index("ep")
    core = me % 2
    x = (me // 2) % SIDE
    y = (me // (2 * SIDE)) % SIDE
    z = me // (2 * SIDE * SIDE)
    return core, (z, y, x)


def device_at(core, spot):
    z, y, x = spot
    return (((z * SIDE + y) * SIDE + x) * 2 + core,)


def moved(spot, dim, value):
    return tuple(value if d == dim else spot[d] for d in range(3))


def shifted(spot, dim, offset):
    return moved(spot, dim, (spot[dim] + offset + SIDE) % SIDE)


def columns(k):
    return pl.ds(CHUNKS[k][0], CHUNKS[k][1])


def remote(src, dst, send, recv, target):
    return pltpu.make_async_remote_copy(
        src_ref=src, dst_ref=dst, send_sem=send, recv_sem=recv, device_id=target, device_id_type=MESH
    )


def entry_signal(core, spot):
    barrier = pltpu.get_barrier_semaphore()
    for offset in range(SIDE):
        pl.semaphore_signal(
            barrier, inc=1, device_id=device_at(1 - core, shifted(spot, 2, offset)), device_id_type=MESH
        )
    for dim in range(3):
        for offset in range(1, SIDE):
            pl.semaphore_signal(
                barrier, inc=1, device_id=device_at(core, shifted(spot, dim, offset)), device_id_type=MESH
            )


def entry_wait():
    pl.semaphore_wait(pltpu.get_barrier_semaphore(), 3 * (SIDE - 1) + SIDE)


PROJ = 256
HALF = 128
WEIGHT_ORDER = ((1, 0), (0, 1))
NT = (((1,), (1,)), ((), ()))
GROUP = 4
HEAD_LANES = 64
PEERS = SIDE - 1
PIECES = (1, 3, 2)
LINE = tuple((offset, flip) for offset in range(SIDE) for flip in range(2))[1:]


def spread_heads(pairs):
    lane = lax.broadcasted_iota(jnp.int32, (8, 2 * HEAD_LANES), 1)
    low = lane < HEAD_LANES
    first, second = pairs[:8], pairs[8:]
    return jnp.concatenate(
        [
            jnp.where(low, first, 0.0),
            jnp.where(low, pltpu.roll(first, HEAD_LANES, 1), 0.0),
            jnp.where(low, 0.0, pltpu.roll(second, HEAD_LANES, 1)),
            jnp.where(low, 0.0, second),
        ],
        axis=0,
    )


def pair_heads(heads):
    lane = lax.broadcasted_iota(jnp.int32, (8, 2 * HEAD_LANES), 1)
    low = lane < HEAD_LANES
    first = jnp.where(low, heads[:8], pltpu.roll(heads[8:16], HEAD_LANES, 1))
    second = jnp.where(low, pltpu.roll(heads[16:24], HEAD_LANES, 1), heads[24:])
    return jnp.concatenate([first, second], axis=0)


def attend_some(first, count, lengths_ref, keys_ref, values_ref, gates_ref, pairs_ref, fresh_ref, gate_ref, mixed_ref):
    slots = keys_ref.shape[1]
    place = lax.broadcasted_iota(jnp.int32, (2, slots), 1)
    column = lax.broadcasted_iota(jnp.int32, (2, ROWS), 1)
    state = []
    for step in range(count):
        b = first + step
        queries = spread_heads(pairs_ref[b])
        scores = lax.dot_general(
            queries.astype(BF16), keys_ref[b], NT, preferred_element_type=F32
        )
        length = lengths_ref[b]
        sums = gates_ref[b]
        latest = jnp.sum(jnp.where(place == length - 1, sums, 0.0), axis=1, keepdims=True)
        fresh_gate = jnp.sum(jnp.where(column == b, gate_ref[...], 0.0), axis=1, keepdims=True)
        offsets = jnp.where(place < length, latest - sums + fresh_gate, -jnp.inf)
        wide = jnp.concatenate(
            [jnp.broadcast_to(offsets[:1], (16, slots)), jnp.broadcast_to(offsets[1:], (16, slots))], axis=0
        )
        scores = scores + wide
        fresh = fresh_ref[pl.ds(b, 1), :]
        own = jnp.sum(queries * fresh[:, : 2 * HEAD_LANES], axis=1, keepdims=True)
        state.append((scores, own, fresh[:, 2 * HEAD_LANES :]))
    for step, (scores, own, fresh_value) in enumerate(state):
        b = first + step
        highest = jnp.maximum(jnp.max(scores, axis=1, keepdims=True), own)
        past = jnp.exp(scores - highest)
        own = jnp.exp(own - highest)
        ratio = 1.0 / (jnp.sum(past, axis=1, keepdims=True) + own)
        weights = (past * ratio).astype(BF16)
        own_weight = (own * ratio).astype(BF16).astype(F32)
        mixed = jnp.dot(weights, values_ref[b], preferred_element_type=F32) + own_weight * fresh_value
        mixed_ref[b] = pair_heads(mixed)


class Transfers:
    def __init__(self):
        self.started = []

    def go(self, copy):
        copy.start()
        self.started.append(copy)

    def drain(self):
        for copy in self.started:
            copy.wait_send()


class Spread:
    def __init__(self, moves, view, core, spot, first, second, send1, recv1, send2, recv2):
        self.moves, self.view, self.core, self.spot = moves, view, core, spot
        self.first, self.second = first, second
        self.send1, self.recv1, self.send2, self.recv2 = send1, recv1, send2, recv2

    def near_copy(self, offset, source, target):
        region = self.view(source)
        return remote(region, region, self.send1.at[offset - 1], self.recv1.at[offset - 1], device_at(self.core, target))

    def far_copy(self, offset, piece, source, target):
        region = self.view(shifted(source, self.first, -piece))
        return remote(
            region, region, self.send2.at[offset - 1, piece], self.recv2.at[offset - 1, piece],
            device_at(self.core, target),
        )

    def far_start(self, piece):
        for offset in PIECES:
            self.moves.go(self.far_copy(offset, piece, self.spot, shifted(self.spot, self.second, offset)))

    def start(self):
        for offset in PIECES:
            self.moves.go(self.near_copy(offset, self.spot, shifted(self.spot, self.first, offset)))
        self.far_start(0)

    def relay(self, offset):
        self.near_copy(offset, shifted(self.spot, self.first, -offset), self.spot).wait_recv()
        self.far_start(offset)

    def far_arrive(self, offset):
        source = shifted(self.spot, self.second, -offset)
        for piece in range(SIDE):
            self.far_copy(offset, piece, source, self.spot).wait_recv()


def step_kernel(
    lengths_hbm, tokens_hbm, keys_hbm, values_hbm, gates_hbm, query_hbm, key_hbm, value_hbm, forget_hbm, ow_hbm,
    routes_hbm, shares_hbm, gate_hbm, up_hbm, down_hbm, dgate_hbm, dup_hbm, ddown_hbm,
    scale_hbm, gain_hbm, bias_hbm, out_ref,
    lengths_ref, tokens_ref, keys_ref, values_ref, gates_ref, wq_ref, wkv_ref, forget_ref, ow_ref, wo_ref,
    routes_ref, shares_ref, scale_ref, gain_ref, bias_ref,
    pairs_ref, mixed_ref, fresh_ref, newgate_ref, line_ref, sent_ref, back_ref, settled_ref,
    rows_ref, wg_ref, wu_ref, wd_ref, dense_ref, factor_ref, hidden_ref, part_ref, r0_ref, r1_ref, r2_ref, s1_ref, s2_ref,
    asem, wsem, swsend, swrecv, xsend, xrecv, w1send, w1recv, w2send, w2recv,
    lsend, lrecv, bsend, brecv,
    g0send, g0recv, g1send, g1recv, g2send, g2recv,
    rsend, rrecv, r1send, r1recv, r2send, r2recv,
):
    core, spot = position()
    partner = device_at(1 - core, spot)
    entry_signal(core, spot)
    depth = WIDTH // GROUP
    first_loads = [(ow_hbm, ow_ref)]
    small = [
        (tokens_hbm, tokens_ref),
        (forget_hbm, forget_ref),
        (key_hbm, wkv_ref.at[:, pl.ds(0, 128)]),
        (value_hbm, wkv_ref.at[:, pl.ds(128, 128)]),
    ]
    wide = [(query_hbm.at[pl.ds(i * depth, depth)], wq_ref.at[pl.ds(i * depth, depth)]) for i in range(GROUP)]
    cache = [
        (keys_hbm, keys_ref), (values_hbm, values_ref), (gates_hbm, gates_ref), (lengths_hbm, lengths_ref),
        (gain_hbm, gain_ref), (bias_hbm, bias_ref), (scale_hbm, scale_ref),
        (routes_hbm, routes_ref), (shares_hbm, shares_ref),
    ]
    tables = ((gate_hbm, wg_ref), (up_hbm, wu_ref), (down_hbm, wd_ref))
    dense = (dgate_hbm, dup_hbm, ddown_hbm)
    shard = [(hbm, ref.at[core, pl.ds(0, FFE)]) for hbm, ref in tables]
    shard += [(hbm, dense_ref.at[core, i]) for i, hbm in enumerate(dense)]
    count = 0
    groups = []
    for group in (first_loads, small, wide, cache, shard):
        copies = []
        for source, target in group:
            copies.append(pltpu.make_async_copy(source, target, asem.at[count]))
            count += 1
        groups.append(copies)
    first_loads, small, wide, cache, shard = groups
    for load in first_loads + small + wide + cache:
        load.start()

    moves = Transfers()
    me = spot[2] * 2 + core

    def swap_copy(table, part, owner):
        hbm, ref = tables[table]
        size = FFE // 4
        here = pl.ds(part * size, size)
        return remote(
            hbm.at[here], ref.at[owner, here], swsend.at[table * 4 + part], swrecv.at[table * 4 + part], partner
        )

    def swap_dense(i, owner):
        return remote(dense[i], dense_ref.at[owner, i], swsend.at[12 + i], swrecv.at[12 + i], partner)

    def swap_start(table):
        for part in range(4):
            moves.go(swap_copy(table, part, core))
        moves.go(swap_dense(table, core))

    def line_target(offset, flip, sign=1):
        return (core if flip == 0 else 1 - core), shifted(spot, 2, sign * offset)

    def block_copy(index, from_core, source, to_core, target):
        z, y, x = source
        here = pl.multiple_of((target[2] * 2 + to_core) * PROJ, PROJ)
        return remote(
            ow_ref.at[:, pl.ds(here, PROJ)], wo_ref.at[z, y, x, from_core], xsend.at[index], xrecv.at[index],
            device_at(to_core, target),
        )

    for load in first_loads:
        load.wait()
    wo_ref[spot[0], spot[1], spot[2], core] = ow_ref[:, pl.ds(pl.multiple_of(me * PROJ, PROJ), PROJ)]
    entry_wait()
    for index, (offset, flip) in enumerate(LINE):
        moves.go(block_copy(index, core, spot, *line_target(offset, flip)))
    for load in shard:
        load.start()

    def weight_view(k):
        def view(source):
            return wo_ref.at[
                source[0], source[1], pl.ds(0, SIDE), pl.ds(0, 2), pl.ds(0, 2 * ROWS), pl.ds(k * HALF, HALF)
            ]

        return view

    weights = [
        Spread(
            moves, weight_view(k), core, spot, *WEIGHT_ORDER[k],
            w1send.at[k], w1recv.at[k], w2send.at[k], w2recv.at[k],
        )
        for k in range(2)
    ]

    for load in small:
        load.wait()
    tokens = tokens_ref[...]
    fresh_ref[...] = jnp.dot(tokens, wkv_ref[...], preferred_element_type=F32).astype(BF16).astype(F32)
    raw = lax.dot_general(forget_ref[...], tokens, NT, preferred_element_type=F32)
    newgate_ref[...] = jnp.minimum(raw, 0.0) - jnp.log1p(jnp.exp(-jnp.abs(raw)))
    query = jnp.zeros((ROWS, WIDTH), F32)
    for i in range(GROUP):
        wide[i].wait()
        query = query + jnp.dot(
            tokens[:, i * depth : (i + 1) * depth], wq_ref[i * depth : (i + 1) * depth, :], preferred_element_type=F32
        )
    query = query.astype(BF16).astype(F32) * HEAD_LANES**-0.5
    flat = pairs_ref.reshape(ROWS * 16, 128)
    for i in range(16):
        flat[pl.ds(i, ROWS, stride=16), :] = query[:, 128 * i : 128 * (i + 1)]
    for index, (offset, flip) in enumerate(LINE):
        from_core, source = line_target(offset, flip, -1)
        block_copy(index, from_core, source, core, spot).wait_recv()
    for weight in weights:
        weight.start()
    swap_start(0)
    for load in cache:
        load.wait()

    def some(i, carry):
        attend_some(
            i * ATTEND, ATTEND, lengths_ref, keys_ref, values_ref, gates_ref, pairs_ref, fresh_ref, newgate_ref,
            mixed_ref,
        )
        return carry

    lax.fori_loop(0, ROWS // ATTEND, some, 0)
    flat = mixed_ref.reshape(ROWS * 16, 128)
    attended = jnp.concatenate([flat[pl.ds(i, ROWS, stride=16), :] for i in range(16)], axis=1).astype(BF16)
    line_ref[spot[2], core] = attended

    def line_copy(index, from_core, source, to_core, target):
        here = line_ref.at[source[2], from_core]
        return remote(here, here, lsend.at[index], lrecv.at[index], device_at(to_core, target))

    for index, (offset, flip) in enumerate(LINE):
        moves.go(line_copy(index, core, spot, *line_target(offset, flip)))
    for offset in PIECES:
        for weight in weights:
            weight.relay(offset)
    swap_start(1)
    swap_start(2)

    expert = lax.axis_index("ep") // (2 * SIDE * SIDE * SIDE // EXPERTS)
    picked = jnp.where(routes_ref[...] == expert, shares_ref[...], 0.0)
    factor = jnp.sum(picked, axis=0, keepdims=True)
    turned = jnp.transpose(jnp.broadcast_to(factor, (8, factor.shape[1])))
    factor_ref[...] = turned.reshape(factor_ref.shape)

    for index, (offset, flip) in enumerate(LINE):
        from_core, source = line_target(offset, flip, -1)
        line_copy(index, from_core, source, core, spot).wait_recv()
    for offset in PIECES:
        for weight in weights:
            weight.far_arrive(offset)
    lines = line_ref.reshape(2 * SIDE * ROWS, WIDTH)[...]
    sent_ref.reshape(2 * SIDE * ROWS, PROJ)[...] = jnp.dot(
        lines, wo_ref.reshape(WIDTH, PROJ)[...], preferred_element_type=F32
    )

    def back_copy(index, from_core, source, to_core, target):
        return remote(
            sent_ref.at[target[2], to_core], back_ref.at[source[2], from_core], bsend.at[index], brecv.at[index],
            device_at(to_core, target),
        )

    for index, (offset, flip) in enumerate(LINE):
        moves.go(back_copy(index, core, spot, *line_target(offset, flip)))
    back_ref[spot[2], core] = sent_ref[spot[2], core]
    for index, (offset, flip) in enumerate(LINE):
        from_core, source = line_target(offset, flip, -1)
        back_copy(index, from_core, source, core, spot).wait_recv()
    projected = jnp.concatenate([back_ref[i // 2, i % 2] for i in range(2 * SIDE)], axis=1)
    settled = norm_rows(residual_scale * tokens.astype(F32) + projected, gain_ref[0:1, :], bias_ref[0:1, :])
    settled_ref[...] = settled
    rows_ref[spot] = settled

    def row_view(k):
        gone = GATHER_ORDER[k][0]

        def view(source):
            where = tuple(pl.ds(0, SIDE) if d == gone else source[d] for d in range(3))
            return rows_ref.at[where + (pl.ds(0, ROWS), columns(k))]

        return view

    def first_copy(k, offset, source, target):
        region = rows_ref.at[source + (pl.ds(0, ROWS), columns(k))]
        return remote(region, region, g0send.at[k, offset - 1], g0recv.at[k, offset - 1], device_at(core, target))

    for offset in PIECES:
        for k in range(3):
            moves.go(first_copy(k, offset, spot, shifted(spot, GATHER_ORDER[k][0], offset)))

    pad = jnp.zeros((FFP - FFE - FFD, WIDTH), BF16)

    def dense_rows(slot):
        for i, ref in ((0, wg_ref), (1, wu_ref), (2, wd_ref)):
            value = dense_ref[slot, i]
            if i == 2:
                value = (value.astype(F32) * scale_ref[...]).astype(BF16)
            ref[slot, FFE:, :] = jnp.concatenate([value, pad], axis=0)

    for load in shard:
        load.wait()
    dense_rows(core)
    spreads = [
        Spread(
            moves, row_view(k), core, spot, *GATHER_ORDER[k][1:],
            g1send.at[k], g1recv.at[k], g2send.at[k], g2recv.at[k],
        )
        for k in range(3)
    ]
    for k in range(3):
        for offset in PIECES:
            first_copy(k, offset, shifted(spot, GATHER_ORDER[k][0], -offset), spot).wait_recv()
        spreads[k].start()
    for offset in PIECES:
        for k in range(3):
            spreads[k].relay(offset)
    for table in range(3):
        for part in range(4):
            swap_copy(table, part, 1 - core).wait_recv()
        swap_dense(table, 1 - core).wait_recv()
    dense_rows(1 - core)
    for offset in PIECES:
        for k in range(3):
            spreads[k].far_arrive(offset)

    plane_rows = SIDE * SIDE * ROWS
    block = 2 * plane_rows
    lane = lax.broadcasted_iota(jnp.int32, (1, 2 * FFP), 1) % FFP
    wg_all, wu_all, wd_all = (ref.reshape(2 * FFP, WIDTH) for ref in (wg_ref, wu_ref, wd_ref))

    def plane(offset):
        return shifted(spot, 0, offset)[0]

    def hidden_block(i, carry):
        pair = (plane(2 + i), plane(1 - i))
        x = jnp.concatenate([rows_ref.at[p].reshape(plane_rows, WIDTH)[...] for p in pair], axis=0)
        gate = lax.dot_general(x, wg_all[...], NT, preferred_element_type=F32)
        up = lax.dot_general(x, wu_all[...], NT, preferred_element_type=F32)
        weight = jnp.concatenate(
            [factor_ref[pl.ds(p * SIDE * SIDE, SIDE * SIDE), core].reshape(plane_rows, 8)[:, :1] for p in pair], axis=0
        )
        weight = jnp.where(lane < FFE, weight, 1.0)
        hidden_ref[...] = (gate * jax.nn.sigmoid(gate) * up * weight).astype(BF16)
        return carry

    def down(i, k):
        here = span(k)
        value = jnp.dot(hidden_ref[...], wd_all[:, here], preferred_element_type=F32).astype(BF16)
        for n, p in enumerate((plane(2 + i), plane(1 - i))):
            part_ref.at[p].reshape(plane_rows, WIDTH)[:, here] = value[n * plane_rows : (n + 1) * plane_rows]

    def span(k):
        return pl.ds(REDUCE_CHUNKS[k][0], REDUCE_CHUNKS[k][1])

    def dims_of(k):
        return GATHER_ORDER[k][::-1]

    def cell(ref, lead, k, phase, fixed):
        gone = dims_of(k)[:phase]
        where = tuple(fixed.get(d, pl.ds(0, SIDE)) for d in range(3) if d not in gone)
        return ref.at[lead + where + (pl.ds(0, ROWS), span(k))]

    def send0(k, offset, piece, target):
        a, b, _ = dims_of(k)
        line = (spot[b] + piece) % SIDE
        return remote(
            cell(part_ref, (), k, 0, {a: target[a], b: line}), cell(r0_ref, (offset - 1,), k, 1, {b: line}),
            rsend.at[k, offset - 1, piece], rrecv.at[k, offset - 1, piece], device_at(core, target),
        )

    def send1(k, offset, target):
        b = dims_of(k)[1]
        return remote(
            cell(s1_ref, (), k, 1, {b: target[b]}), cell(r1_ref, (offset - 1,), k, 2, {}),
            r1send.at[k, offset - 1], r1recv.at[k, offset - 1], device_at(core, target),
        )

    def send2(k, offset, target):
        c = dims_of(k)[2]
        return remote(
            cell(s2_ref, (), k, 2, {c: target[c]}), cell(r2_ref, (offset - 1,), k, 3, {}),
            r2send.at[k, offset - 1], r2recv.at[k, offset - 1], device_at(core, target),
        )

    def send_part(k, offsets, pieces):
        for piece in pieces:
            for offset in offsets:
                moves.go(send0(k, offset, piece, shifted(spot, dims_of(k)[0], offset)))

    def sum_part(k, piece):
        a, b, _ = dims_of(k)
        line = (spot[b] + piece) % SIDE
        total = cell(part_ref, (), k, 0, {a: spot[a], b: line})[...].astype(F32)
        for offset in PIECES:
            send0(k, offset, piece, spot).wait_recv()
            total = total + cell(r0_ref, (offset - 1,), k, 1, {b: line})[...].astype(F32)
        cell(s1_ref, (), k, 1, {b: line})[...] = total.astype(BF16)
        if piece:
            moves.go(send1(k, piece, shifted(spot, b, piece)))

    order = (2, 1, 3, 0)
    hidden_block(0, 0)
    down(0, 0)
    send_part(0, (1, 2), order)
    down(0, 2)
    send_part(2, PIECES, (2, 1))
    down(0, 1)
    hidden_block(1, 0)
    down(1, 1)
    send_part(1, PIECES, order)
    down(1, 0)
    send_part(0, (3,), order)
    down(1, 2)
    send_part(2, PIECES, (3, 0))
    for k, piece in ((2, 2), (2, 1), (1, 2), (0, 2), (1, 1), (0, 1), (2, 3), (1, 3), (0, 3), (2, 0), (1, 0), (0, 0)):
        sum_part(k, piece)
    for k in range(3):
        b, c = dims_of(k)[1:]
        total = cell(s1_ref, (), k, 1, {b: spot[b]})[...].astype(F32)
        for offset in PIECES:
            send1(k, offset, spot).wait_recv()
            total = total + cell(r1_ref, (offset - 1,), k, 2, {})[...].astype(F32)
        cell(s2_ref, (), k, 2, {})[...] = total.astype(BF16)
        for offset in PIECES:
            moves.go(send2(k, offset, shifted(spot, c, offset)))
    sums = []
    for k in range(3):
        c = dims_of(k)[2]
        total = cell(s2_ref, (), k, 2, {c: spot[c]})[...].astype(F32)
        for offset in PIECES:
            send2(k, offset, spot).wait_recv()
            total = total + cell(r2_ref, (offset - 1,), k, 3, {})[...].astype(F32)
        sums.append(total)
    ffn_sum = jnp.concatenate(sums, axis=-1)
    out_ref[...] = norm_rows(
        residual_scale * settled_ref[...].astype(F32) + ffn_sum, gain_ref[1:2, :], bias_ref[1:2, :]
    )
    moves.drain()


def step_call(*operands):
    vmem = pl.BlockSpec(memory_space=pltpu.VMEM)
    hbm = pl.BlockSpec(memory_space=pltpu.HBM)
    sem = pltpu.SemaphoreType.DMA
    cube = (SIDE, SIDE, SIDE, ROWS, WIDTH)
    slots = operands[2].shape[1]
    line = len(LINE)
    return pl.pallas_call(
        step_kernel,
        out_shape=jax.ShapeDtypeStruct((ROWS, WIDTH), BF16),
        in_specs=[hbm] * len(operands),
        out_specs=vmem,
        scratch_shapes=[
            pltpu.SMEM((ROWS,), jnp.int32),
            pltpu.VMEM((ROWS, WIDTH), BF16),
            pltpu.VMEM((ROWS, slots, 128), BF16),
            pltpu.VMEM((ROWS, slots, 128), BF16),
            pltpu.VMEM((ROWS, 2, slots), F32),
            pltpu.VMEM((WIDTH, WIDTH), BF16),
            pltpu.VMEM((WIDTH, 256), BF16),
            pltpu.VMEM((2, WIDTH), BF16),
            pltpu.VMEM((2 * ROWS, WIDTH), BF16),
            pltpu.VMEM((SIDE, SIDE, SIDE, 2, 2 * ROWS, PROJ), BF16),
            pltpu.VMEM((2, 2 * SIDE**3 * ROWS), jnp.int32),
            pltpu.VMEM((2, 2 * SIDE**3 * ROWS), F32),
            pltpu.VMEM((1, WIDTH), F32),
            pltpu.VMEM((2, WIDTH), F32),
            pltpu.VMEM((2, WIDTH), F32),
            pltpu.VMEM((ROWS, 16, 128), F32),
            pltpu.VMEM((ROWS, 16, 128), F32),
            pltpu.VMEM((ROWS, 256), F32),
            pltpu.VMEM((2, ROWS), F32),
            pltpu.VMEM((SIDE, 2, ROWS, WIDTH), BF16),
            pltpu.VMEM((SIDE, 2, ROWS, PROJ), F32),
            pltpu.VMEM((SIDE, 2, ROWS, PROJ), F32),
            pltpu.VMEM((ROWS, WIDTH), BF16),
            pltpu.VMEM(cube, BF16),
            pltpu.VMEM((2, FFP, WIDTH), BF16),
            pltpu.VMEM((2, FFP, WIDTH), BF16),
            pltpu.VMEM((2, FFP, WIDTH), BF16),
            pltpu.VMEM((2, 3, FFD, WIDTH), BF16),
            pltpu.VMEM((SIDE**3, 2, ROWS, 8), F32),
            pltpu.VMEM((2 * SIDE * SIDE * ROWS, 2 * FFP), BF16),
            pltpu.VMEM(cube, BF16),
            pltpu.VMEM((PEERS,) + cube[1:], BF16),
            pltpu.VMEM((PEERS,) + cube[2:], BF16),
            pltpu.VMEM((PEERS,) + cube[3:], BF16),
            pltpu.VMEM(cube[1:], BF16),
            pltpu.VMEM(cube[2:], BF16),
            sem((24,)), sem((1,)), sem((15,)), sem((15,)),
            sem((line,)), sem((line,)),
            sem((2, PEERS)), sem((2, PEERS)), sem((2, PEERS, SIDE)), sem((2, PEERS, SIDE)),
            sem((line,)), sem((line,)), sem((line,)), sem((line,)),
            sem((3, PEERS)), sem((3, PEERS)),
            sem((3, PEERS)), sem((3, PEERS)), sem((3, PEERS, SIDE)), sem((3, PEERS, SIDE)),
            sem((3, PEERS, SIDE)), sem((3, PEERS, SIDE)),
            sem((3, PEERS)), sem((3, PEERS)), sem((3, PEERS)), sem((3, PEERS)),
        ],
        compiler_params=pltpu.CompilerParams(
            collective_id=0, has_side_effects=True, vmem_limit_bytes=60 * 2**20
        ),
        name="step",
    )(*operands)


def local(
    tokens,
    cache_keys,
    cache_values,
    cum_gates,
    lengths,
    query_weight,
    key_weight,
    value_weight,
    forget_weight,
    out_weight,
    norm_gain,
    norm_bias,
    dense_gate_weight,
    dense_up_weight,
    dense_down_weight,
    dense_scale,
    expert_gate_weight,
    expert_up_weight,
    expert_down_weight,
    routes,
    route_weights,
):
    return step_call(
        lengths,
        tokens,
        cache_keys,
        cache_values,
        jnp.transpose(cum_gates, (0, 2, 1)),
        query_weight,
        key_weight,
        value_weight,
        jnp.transpose(forget_weight),
        out_weight,
        jnp.transpose(routes),
        jnp.transpose(route_weights),
        jnp.transpose(expert_gate_weight),
        jnp.transpose(expert_up_weight),
        expert_down_weight,
        jnp.transpose(dense_gate_weight),
        jnp.transpose(dense_up_weight),
        dense_down_weight,
        dense_scale.reshape(1, -1),
        norm_gain,
        norm_bias,
    )


def solution(mesh):
    return jax.shard_map(
        local,
        mesh=mesh,
        in_specs=(
            P("ep", None),
            P("ep", None, None),
            P("ep", None, None),
            P("ep", None, None),
            P("ep"),
            P(),
            P(),
            P(),
            P(),
            P("ep", None),
            P(),
            P(),
            P(None, "ep"),
            P(None, "ep"),
            P("ep", None),
            P(),
            P(None, "ep"),
            P(None, "ep"),
            P("ep", None),
            P(),
            P(),
        ),
        out_specs=P("ep", None),
        check_vma=False,
    )
```

```python
import functools

import jax
import jax.numpy as jnp
from jax import lax
from jax.experimental import pallas as pl
from jax.experimental.pallas import tpu as pltpu
from jax.sharding import PartitionSpec as P

MESH = pl.DeviceIdType.MESH
F32 = jnp.float32
BF16 = jnp.bfloat16
SIDE = 4
ROWS = 8
WIDTH = 2048
EXPERTS = 8
FFE = 448
FFD = 44
FFP = 512
CHUNKS = ((0, 768), (768, 640), (1408, 640))
REDUCE_CHUNKS = ((0, 768), (768, 512), (1280, 768))
GATHER_ORDER = ((2, 1, 0), (0, 2, 1), (1, 0, 2))
ATTEND = 4
residual_scale = 1.4142135
norm_eps = 1e-05


def norm_rows(values, gain_row, shift_row):
    centre = jnp.mean(values, axis=-1, keepdims=True)
    centred = values - centre
    spread = jnp.mean(centred * centred, axis=-1, keepdims=True)
    return (centred * lax.rsqrt(spread + norm_eps) * gain_row + shift_row).astype(BF16)


def position():
    me = lax.axis_index("ep")
    core = me % 2
    x = (me // 2) % SIDE
    y = (me // (2 * SIDE)) % SIDE
    z = me // (2 * SIDE * SIDE)
    return core, (z, y, x)


def device_at(core, spot):
    z, y, x = spot
    return (((z * SIDE + y) * SIDE + x) * 2 + core,)


def moved(spot, dim, value):
    return tuple(value if d == dim else spot[d] for d in range(3))


def shifted(spot, dim, offset):
    return moved(spot, dim, (spot[dim] + offset + SIDE) % SIDE)


def columns(k):
    return pl.ds(CHUNKS[k][0], CHUNKS[k][1])


def remote(src, dst, send, recv, target):
    return pltpu.make_async_remote_copy(
        src_ref=src, dst_ref=dst, send_sem=send, recv_sem=recv, device_id=target, device_id_type=MESH
    )


def entry_signal(core, spot):
    barrier = pltpu.get_barrier_semaphore()
    for offset in range(SIDE):
        pl.semaphore_signal(
            barrier, inc=1, device_id=device_at(1 - core, shifted(spot, 2, offset)), device_id_type=MESH
        )
    for dim in range(3):
        for offset in range(1, SIDE):
            pl.semaphore_signal(
                barrier, inc=1, device_id=device_at(core, shifted(spot, dim, offset)), device_id_type=MESH
            )


def entry_wait():
    pl.semaphore_wait(pltpu.get_barrier_semaphore(), 3 * (SIDE - 1) + SIDE)


PROJ = 256
HALF = 128
WEIGHT_ORDER = ((1, 0), (0, 1))
NT = (((1,), (1,)), ((), ()))
GROUP = 4
HEAD_LANES = 64
PEERS = SIDE - 1
PIECES = (1, 3, 2)
FAR_FIRST = (2, 1, 3)
LINE = tuple((offset, flip) for offset in FAR_FIRST + (0,) for flip in range(2) if offset or flip)


def spread_heads(pairs):
    lane = lax.broadcasted_iota(jnp.int32, (8, 2 * HEAD_LANES), 1)
    low = lane < HEAD_LANES
    first, second = pairs[:8], pairs[8:]
    return jnp.concatenate(
        [
            jnp.where(low, first, 0.0),
            jnp.where(low, pltpu.roll(first, HEAD_LANES, 1), 0.0),
            jnp.where(low, 0.0, pltpu.roll(second, HEAD_LANES, 1)),
            jnp.where(low, 0.0, second),
        ],
        axis=0,
    )


def pair_heads(heads):
    lane = lax.broadcasted_iota(jnp.int32, (8, 2 * HEAD_LANES), 1)
    low = lane < HEAD_LANES
    first = jnp.where(low, heads[:8], pltpu.roll(heads[8:16], HEAD_LANES, 1))
    second = jnp.where(low, pltpu.roll(heads[16:24], HEAD_LANES, 1), heads[24:])
    return jnp.concatenate([first, second], axis=0)


def attend_some(first, count, lengths_ref, keys_ref, values_ref, gates_ref, pairs_ref, fresh_ref, gate_ref, mixed_ref):
    slots = keys_ref.shape[1]
    place = lax.broadcasted_iota(jnp.int32, (2, slots), 1)
    column = lax.broadcasted_iota(jnp.int32, (2, ROWS), 1)
    state = []
    for step in range(count):
        b = first + step
        queries = spread_heads(pairs_ref[b])
        scores = lax.dot_general(
            queries.astype(BF16), keys_ref[b], NT, preferred_element_type=F32
        )
        length = lengths_ref[b]
        sums = gates_ref[b]
        latest = jnp.sum(jnp.where(place == length - 1, sums, 0.0), axis=1, keepdims=True)
        fresh_gate = jnp.sum(jnp.where(column == b, gate_ref[...], 0.0), axis=1, keepdims=True)
        offsets = jnp.where(place < length, latest - sums + fresh_gate, -jnp.inf)
        wide = jnp.concatenate(
            [jnp.broadcast_to(offsets[:1], (16, slots)), jnp.broadcast_to(offsets[1:], (16, slots))], axis=0
        )
        scores = scores + wide
        fresh = fresh_ref[pl.ds(b, 1), :]
        own = jnp.sum(queries * fresh[:, : 2 * HEAD_LANES], axis=1, keepdims=True)
        state.append((scores, own, fresh[:, 2 * HEAD_LANES :]))
    for step, (scores, own, fresh_value) in enumerate(state):
        b = first + step
        highest = jnp.maximum(jnp.max(scores, axis=1, keepdims=True), own)
        past = jnp.exp(scores - highest)
        own = jnp.exp(own - highest)
        ratio = 1.0 / (jnp.sum(past, axis=1, keepdims=True) + own)
        weights = (past * ratio).astype(BF16)
        own_weight = (own * ratio).astype(BF16).astype(F32)
        mixed = jnp.dot(weights, values_ref[b], preferred_element_type=F32) + own_weight * fresh_value
        mixed_ref[b] = pair_heads(mixed)


class Transfers:
    def __init__(self):
        self.started = []

    def go(self, copy):
        copy.start()
        self.started.append(copy)

    def drain(self):
        for copy in self.started:
            copy.wait_send()
        self.started = []


class Spread:
    def __init__(self, moves, view, core, spot, first, second, send1, recv1, send2, recv2):
        self.moves, self.view, self.core, self.spot = moves, view, core, spot
        self.first, self.second = first, second
        self.send1, self.recv1, self.send2, self.recv2 = send1, recv1, send2, recv2

    def near_copy(self, offset, source, target):
        region = self.view(source)
        return remote(region, region, self.send1.at[offset - 1], self.recv1.at[offset - 1], device_at(self.core, target))

    def far_copy(self, offset, piece, source, target):
        region = self.view(shifted(source, self.first, -piece))
        return remote(
            region, region, self.send2.at[offset - 1, piece], self.recv2.at[offset - 1, piece],
            device_at(self.core, target),
        )

    def far_start(self, piece):
        for offset in FAR_FIRST:
            self.moves.go(self.far_copy(offset, piece, self.spot, shifted(self.spot, self.second, offset)))

    def start(self):
        for offset in PIECES:
            self.moves.go(self.near_copy(offset, self.spot, shifted(self.spot, self.first, offset)))
        self.far_start(0)

    def relay(self, offset):
        self.near_copy(offset, shifted(self.spot, self.first, -offset), self.spot).wait_recv()
        self.far_start(offset)

    def far_arrive(self, offset):
        source = shifted(self.spot, self.second, -offset)
        for piece in range(SIDE):
            self.far_copy(offset, piece, source, self.spot).wait_recv()


def step_kernel(
    lengths_hbm, tokens_hbm, keys_hbm, values_hbm, gates_hbm, query_hbm, key_hbm, value_hbm, forget_hbm, ow_hbm,
    routes_hbm, shares_hbm, gate_hbm, up_hbm, down_hbm, dgate_hbm, dup_hbm, ddown_hbm,
    scale_hbm, gain_hbm, bias_hbm, out_ref,
    lengths_ref, tokens_ref, keys_ref, values_ref, gates_ref, wq_ref, wkv_ref, forget_ref, ow_ref, wo_ref,
    routes_ref, shares_ref, scale_ref, gain_ref, bias_ref,
    pairs_ref, mixed_ref, fresh_ref, newgate_ref, line_ref, sent_ref, back_ref, settled_ref,
    rows_ref, wg_ref, wu_ref, wd_ref, dense_ref, factor_ref, hidden_ref, part_ref, r0_ref, r1_ref, r2_ref, s1_ref, s2_ref,
    asem, wsem, swsend, swrecv, xsend, xrecv, w1send, w1recv, w2send, w2recv,
    lsend, lrecv, bsend, brecv,
    g0send, g0recv, g1send, g1recv, g2send, g2recv,
    rsend, rrecv, r1send, r1recv, r2send, r2recv,
):
    core, spot = position()
    partner = device_at(1 - core, spot)
    entry_signal(core, spot)
    depth = WIDTH // GROUP
    first_loads = [(ow_hbm, ow_ref)]
    small = [
        (tokens_hbm, tokens_ref),
        (forget_hbm, forget_ref),
        (key_hbm, wkv_ref.at[:, pl.ds(0, 128)]),
        (value_hbm, wkv_ref.at[:, pl.ds(128, 128)]),
    ]
    wide = [(query_hbm.at[pl.ds(i * depth, depth)], wq_ref.at[pl.ds(i * depth, depth)]) for i in range(GROUP)]
    cache = [
        (keys_hbm, keys_ref), (values_hbm, values_ref), (gates_hbm, gates_ref), (lengths_hbm, lengths_ref),
        (gain_hbm, gain_ref), (bias_hbm, bias_ref), (scale_hbm, scale_ref),
        (routes_hbm, routes_ref), (shares_hbm, shares_ref),
    ]
    tables = ((gate_hbm, wg_ref), (up_hbm, wu_ref), (down_hbm, wd_ref))
    dense = (dgate_hbm, dup_hbm, ddown_hbm)
    shard = [(hbm, ref.at[core, pl.ds(0, FFE)]) for hbm, ref in tables]
    shard += [(hbm, dense_ref.at[core, i]) for i, hbm in enumerate(dense)]
    count = 0
    groups = []
    for group in (first_loads, small, wide, cache, shard):
        copies = []
        for source, target in group:
            copies.append(pltpu.make_async_copy(source, target, asem.at[count]))
            count += 1
        groups.append(copies)
    first_loads, small, wide, cache, shard = groups
    for load in first_loads + small + wide + cache:
        load.start()

    moves = Transfers()
    me = spot[2] * 2 + core

    def swap_copy(table, part, owner):
        hbm, ref = tables[table]
        size = FFE // 4
        here = pl.ds(part * size, size)
        return remote(
            hbm.at[here], ref.at[owner, here], swsend.at[table * 4 + part], swrecv.at[table * 4 + part], partner
        )

    def swap_dense(i, owner):
        return remote(dense[i], dense_ref.at[owner, i], swsend.at[12 + i], swrecv.at[12 + i], partner)

    def swap_start(table):
        for part in range(4):
            moves.go(swap_copy(table, part, core))
        moves.go(swap_dense(table, core))

    def line_target(offset, flip, sign=1):
        return (core if flip == 0 else 1 - core), shifted(spot, 2, sign * offset)

    def block_copy(index, from_core, source, to_core, target):
        z, y, x = source
        here = pl.multiple_of((target[2] * 2 + to_core) * PROJ, PROJ)
        return remote(
            ow_ref.at[:, pl.ds(here, PROJ)], wo_ref.at[z, y, x, from_core], xsend.at[index], xrecv.at[index],
            device_at(to_core, target),
        )

    for load in first_loads:
        load.wait()
    wo_ref[spot[0], spot[1], spot[2], core] = ow_ref[:, pl.ds(pl.multiple_of(me * PROJ, PROJ), PROJ)]
    entry_wait()
    for index, (offset, flip) in enumerate(LINE):
        moves.go(block_copy(index, core, spot, *line_target(offset, flip)))
    for load in shard:
        load.start()

    def weight_view(k):
        def view(source):
            return wo_ref.at[
                source[0], source[1], pl.ds(0, SIDE), pl.ds(0, 2), pl.ds(0, 2 * ROWS), pl.ds(k * HALF, HALF)
            ]

        return view

    weights = [
        Spread(
            moves, weight_view(k), core, spot, *WEIGHT_ORDER[k],
            w1send.at[k], w1recv.at[k], w2send.at[k], w2recv.at[k],
        )
        for k in range(2)
    ]

    for load in small:
        load.wait()
    tokens = tokens_ref[...]
    fresh_ref[...] = jnp.dot(tokens, wkv_ref[...], preferred_element_type=F32).astype(BF16).astype(F32)
    raw = lax.dot_general(forget_ref[...], tokens, NT, preferred_element_type=F32)
    newgate_ref[...] = jnp.minimum(raw, 0.0) - jnp.log1p(jnp.exp(-jnp.abs(raw)))
    query = jnp.zeros((ROWS, WIDTH), F32)
    for i in range(GROUP):
        wide[i].wait()
        query = query + jnp.dot(
            tokens[:, i * depth : (i + 1) * depth], wq_ref[i * depth : (i + 1) * depth, :], preferred_element_type=F32
        )
    query = query.astype(BF16).astype(F32) * HEAD_LANES**-0.5
    flat = pairs_ref.reshape(ROWS * 16, 128)
    for i in range(16):
        flat[pl.ds(i, ROWS, stride=16), :] = query[:, 128 * i : 128 * (i + 1)]
    for index, (offset, flip) in enumerate(LINE):
        from_core, source = line_target(offset, flip, -1)
        block_copy(index, from_core, source, core, spot).wait_recv()
    for weight in weights:
        weight.start()
    swap_start(0)
    for load in cache:
        load.wait()

    def some(i, carry):
        attend_some(
            i * ATTEND, ATTEND, lengths_ref, keys_ref, values_ref, gates_ref, pairs_ref, fresh_ref, newgate_ref,
            mixed_ref,
        )
        return carry

    lax.fori_loop(0, ROWS // ATTEND, some, 0)
    flat = mixed_ref.reshape(ROWS * 16, 128)
    attended = jnp.concatenate([flat[pl.ds(i, ROWS, stride=16), :] for i in range(16)], axis=1).astype(BF16)
    line_ref[spot[2], core] = attended

    def line_copy(index, from_core, source, to_core, target):
        here = line_ref.at[source[2], from_core]
        return remote(here, here, lsend.at[index], lrecv.at[index], device_at(to_core, target))

    for index, (offset, flip) in enumerate(LINE):
        moves.go(line_copy(index, core, spot, *line_target(offset, flip)))
    for offset in PIECES:
        for weight in weights:
            weight.relay(offset)
    swap_start(1)
    swap_start(2)

    expert = lax.axis_index("ep") // (2 * SIDE * SIDE * SIDE // EXPERTS)
    picked = jnp.where(routes_ref[...] == expert, shares_ref[...], 0.0)
    factor = jnp.sum(picked, axis=0, keepdims=True)
    turned = jnp.transpose(jnp.broadcast_to(factor, (8, factor.shape[1])))
    factor_ref[...] = turned.reshape(factor_ref.shape)

    for index, (offset, flip) in enumerate(LINE):
        from_core, source = line_target(offset, flip, -1)
        line_copy(index, from_core, source, core, spot).wait_recv()
    for offset in PIECES:
        for weight in weights:
            weight.far_arrive(offset)
    lines = line_ref.reshape(2 * SIDE * ROWS, WIDTH)[...]
    sent_ref.reshape(2 * SIDE * ROWS, PROJ)[...] = jnp.dot(
        lines, wo_ref.reshape(WIDTH, PROJ)[...], preferred_element_type=F32
    )

    def back_copy(index, from_core, source, to_core, target):
        return remote(
            sent_ref.at[target[2], to_core], back_ref.at[source[2], from_core], bsend.at[index], brecv.at[index],
            device_at(to_core, target),
        )

    for index, (offset, flip) in enumerate(LINE):
        moves.go(back_copy(index, core, spot, *line_target(offset, flip)))
    back_ref[spot[2], core] = sent_ref[spot[2], core]
    for index, (offset, flip) in enumerate(LINE):
        from_core, source = line_target(offset, flip, -1)
        back_copy(index, from_core, source, core, spot).wait_recv()
    projected = jnp.concatenate([back_ref[i // 2, i % 2] for i in range(2 * SIDE)], axis=1)
    settled = norm_rows(residual_scale * tokens.astype(F32) + projected, gain_ref[0:1, :], bias_ref[0:1, :])
    settled_ref[...] = settled
    rows_ref[spot] = settled

    def row_view(k):
        gone = GATHER_ORDER[k][0]

        def view(source):
            where = tuple(pl.ds(0, SIDE) if d == gone else source[d] for d in range(3))
            return rows_ref.at[where + (pl.ds(0, ROWS), columns(k))]

        return view

    def first_copy(k, offset, source, target):
        region = rows_ref.at[source + (pl.ds(0, ROWS), columns(k))]
        return remote(region, region, g0send.at[k, offset - 1], g0recv.at[k, offset - 1], device_at(core, target))

    for offset in FAR_FIRST:
        for k in range(3):
            moves.go(first_copy(k, offset, spot, shifted(spot, GATHER_ORDER[k][0], offset)))

    pad = jnp.zeros((FFP - FFE - FFD, WIDTH), BF16)

    def dense_rows(slot):
        for i, ref in ((0, wg_ref), (1, wu_ref), (2, wd_ref)):
            value = dense_ref[slot, i]
            if i == 2:
                value = (value.astype(F32) * scale_ref[...]).astype(BF16)
            ref[slot, FFE:, :] = jnp.concatenate([value, pad], axis=0)

    for load in shard:
        load.wait()
    dense_rows(core)
    spreads = [
        Spread(
            moves, row_view(k), core, spot, *GATHER_ORDER[k][1:],
            g1send.at[k], g1recv.at[k], g2send.at[k], g2recv.at[k],
        )
        for k in range(3)
    ]
    for k in range(3):
        for offset in PIECES:
            first_copy(k, offset, shifted(spot, GATHER_ORDER[k][0], -offset), spot).wait_recv()
        spreads[k].start()
    for offset in PIECES:
        for k in range(3):
            spreads[k].relay(offset)
    for table in range(3):
        for part in range(4):
            swap_copy(table, part, 1 - core).wait_recv()
        swap_dense(table, 1 - core).wait_recv()
    dense_rows(1 - core)
    for offset in PIECES:
        for k in range(3):
            spreads[k].far_arrive(offset)

    plane_rows = SIDE * SIDE * ROWS
    block = 2 * plane_rows
    lane = lax.broadcasted_iota(jnp.int32, (1, 2 * FFP), 1) % FFP
    wg_all, wu_all, wd_all = (ref.reshape(2 * FFP, WIDTH) for ref in (wg_ref, wu_ref, wd_ref))

    def plane(offset):
        return shifted(spot, 0, offset)[0]

    def hidden_block(i, carry):
        pair = (plane(2 + i), plane(1 - i))
        x = jnp.concatenate([rows_ref.at[p].reshape(plane_rows, WIDTH)[...] for p in pair], axis=0)
        gate = lax.dot_general(x, wg_all[...], NT, preferred_element_type=F32)
        up = lax.dot_general(x, wu_all[...], NT, preferred_element_type=F32)
        weight = jnp.concatenate(
            [factor_ref[pl.ds(p * SIDE * SIDE, SIDE * SIDE), core].reshape(plane_rows, 8)[:, :1] for p in pair], axis=0
        )
        weight = jnp.where(lane < FFE, weight, 1.0)
        hidden_ref[...] = (gate * jax.nn.sigmoid(gate) * up * weight).astype(BF16)
        return carry

    def down(i, k):
        here = span(k)
        value = jnp.dot(hidden_ref[...], wd_all[:, here], preferred_element_type=F32).astype(BF16)
        for n, p in enumerate((plane(2 + i), plane(1 - i))):
            part_ref.at[p].reshape(plane_rows, WIDTH)[:, here] = value[n * plane_rows : (n + 1) * plane_rows]

    def span(k):
        return pl.ds(REDUCE_CHUNKS[k][0], REDUCE_CHUNKS[k][1])

    def dims_of(k):
        return GATHER_ORDER[k][::-1]

    def cell(ref, lead, k, phase, fixed):
        gone = dims_of(k)[:phase]
        where = tuple(fixed.get(d, pl.ds(0, SIDE)) for d in range(3) if d not in gone)
        return ref.at[lead + where + (pl.ds(0, ROWS), span(k))]

    def send0(k, offset, piece, target):
        a, b, _ = dims_of(k)
        line = (spot[b] + piece) % SIDE
        return remote(
            cell(part_ref, (), k, 0, {a: target[a], b: line}), cell(r0_ref, (offset - 1,), k, 1, {b: line}),
            rsend.at[k, offset - 1, piece], rrecv.at[k, offset - 1, piece], device_at(core, target),
        )

    def send1(k, offset, target):
        b = dims_of(k)[1]
        return remote(
            cell(s1_ref, (), k, 1, {b: target[b]}), cell(r1_ref, (offset - 1,), k, 2, {}),
            r1send.at[k, offset - 1], r1recv.at[k, offset - 1], device_at(core, target),
        )

    def send2(k, offset, target):
        c = dims_of(k)[2]
        return remote(
            cell(s2_ref, (), k, 2, {c: target[c]}), cell(r2_ref, (offset - 1,), k, 3, {}),
            r2send.at[k, offset - 1], r2recv.at[k, offset - 1], device_at(core, target),
        )

    def send_part(k, offsets, pieces):
        for piece in pieces:
            for offset in offsets:
                moves.go(send0(k, offset, piece, shifted(spot, dims_of(k)[0], offset)))

    def sum_part(k, piece):
        a, b, _ = dims_of(k)
        line = (spot[b] + piece) % SIDE
        total = cell(part_ref, (), k, 0, {a: spot[a], b: line})[...].astype(F32)
        for offset in PIECES:
            send0(k, offset, piece, spot).wait_recv()
            total = total + cell(r0_ref, (offset - 1,), k, 1, {b: line})[...].astype(F32)
        cell(s1_ref, (), k, 1, {b: line})[...] = total.astype(BF16)
        if piece:
            moves.go(send1(k, piece, shifted(spot, b, piece)))

    order = (2, 1, 3, 0)
    before = len(moves.started)
    hidden_block(0, 0)
    down(0, 0)
    send_part(0, (2, 1), order)
    down(0, 2)
    send_part(2, FAR_FIRST, (2, 1))
    down(0, 1)
    hidden_block(1, 0)
    down(1, 1)
    send_part(1, FAR_FIRST, order)
    down(1, 0)
    send_part(0, (3,), order)
    down(1, 2)
    early = moves.started[:before]
    moves.started = moves.started[before:]
    send_part(2, FAR_FIRST, (3, 0))
    for copy in early:
        copy.wait_send()
    for k, piece in ((2, 2), (2, 1), (1, 2), (1, 1), (0, 2), (0, 1), (1, 3), (0, 3), (2, 3), (1, 0), (0, 0), (2, 0)):
        sum_part(k, piece)
    for k in range(3):
        b, c = dims_of(k)[1:]
        total = cell(s1_ref, (), k, 1, {b: spot[b]})[...].astype(F32)
        for offset in PIECES:
            send1(k, offset, spot).wait_recv()
            total = total + cell(r1_ref, (offset - 1,), k, 2, {})[...].astype(F32)
        cell(s2_ref, (), k, 2, {})[...] = total.astype(BF16)
        for offset in FAR_FIRST:
            moves.go(send2(k, offset, shifted(spot, c, offset)))
    moves.drain()
    sums = []
    for k in range(3):
        c = dims_of(k)[2]
        total = cell(s2_ref, (), k, 2, {c: spot[c]})[...].astype(F32)
        for offset in PIECES:
            send2(k, offset, spot).wait_recv()
            total = total + cell(r2_ref, (offset - 1,), k, 3, {})[...].astype(F32)
        sums.append(total)
    ffn_sum = jnp.concatenate(sums, axis=-1)
    out_ref[...] = norm_rows(
        residual_scale * settled_ref[...].astype(F32) + ffn_sum, gain_ref[1:2, :], bias_ref[1:2, :]
    )
    moves.drain()


def step_call(*operands):
    vmem = pl.BlockSpec(memory_space=pltpu.VMEM)
    hbm = pl.BlockSpec(memory_space=pltpu.HBM)
    sem = pltpu.SemaphoreType.DMA
    cube = (SIDE, SIDE, SIDE, ROWS, WIDTH)
    slots = operands[2].shape[1]
    line = len(LINE)
    return pl.pallas_call(
        step_kernel,
        out_shape=jax.ShapeDtypeStruct((ROWS, WIDTH), BF16),
        in_specs=[hbm] * len(operands),
        out_specs=vmem,
        scratch_shapes=[
            pltpu.SMEM((ROWS,), jnp.int32),
            pltpu.VMEM((ROWS, WIDTH), BF16),
            pltpu.VMEM((ROWS, slots, 128), BF16),
            pltpu.VMEM((ROWS, slots, 128), BF16),
            pltpu.VMEM((ROWS, 2, slots), F32),
            pltpu.VMEM((WIDTH, WIDTH), BF16),
            pltpu.VMEM((WIDTH, 256), BF16),
            pltpu.VMEM((2, WIDTH), BF16),
            pltpu.VMEM((2 * ROWS, WIDTH), BF16),
            pltpu.VMEM((SIDE, SIDE, SIDE, 2, 2 * ROWS, PROJ), BF16),
            pltpu.VMEM((2, 2 * SIDE**3 * ROWS), jnp.int32),
            pltpu.VMEM((2, 2 * SIDE**3 * ROWS), F32),
            pltpu.VMEM((1, WIDTH), F32),
            pltpu.VMEM((2, WIDTH), F32),
            pltpu.VMEM((2, WIDTH), F32),
            pltpu.VMEM((ROWS, 16, 128), F32),
            pltpu.VMEM((ROWS, 16, 128), F32),
            pltpu.VMEM((ROWS, 256), F32),
            pltpu.VMEM((2, ROWS), F32),
            pltpu.VMEM((SIDE, 2, ROWS, WIDTH), BF16),
            pltpu.VMEM((SIDE, 2, ROWS, PROJ), F32),
            pltpu.VMEM((SIDE, 2, ROWS, PROJ), F32),
            pltpu.VMEM((ROWS, WIDTH), BF16),
            pltpu.VMEM(cube, BF16),
            pltpu.VMEM((2, FFP, WIDTH), BF16),
            pltpu.VMEM((2, FFP, WIDTH), BF16),
            pltpu.VMEM((2, FFP, WIDTH), BF16),
            pltpu.VMEM((2, 3, FFD, WIDTH), BF16),
            pltpu.VMEM((SIDE**3, 2, ROWS, 8), F32),
            pltpu.VMEM((2 * SIDE * SIDE * ROWS, 2 * FFP), BF16),
            pltpu.VMEM(cube, BF16),
            pltpu.VMEM((PEERS,) + cube[1:], BF16),
            pltpu.VMEM((PEERS,) + cube[2:], BF16),
            pltpu.VMEM((PEERS,) + cube[3:], BF16),
            pltpu.VMEM(cube[1:], BF16),
            pltpu.VMEM(cube[2:], BF16),
            sem((24,)), sem((1,)), sem((15,)), sem((15,)),
            sem((line,)), sem((line,)),
            sem((2, PEERS)), sem((2, PEERS)), sem((2, PEERS, SIDE)), sem((2, PEERS, SIDE)),
            sem((line,)), sem((line,)), sem((line,)), sem((line,)),
            sem((3, PEERS)), sem((3, PEERS)),
            sem((3, PEERS)), sem((3, PEERS)), sem((3, PEERS, SIDE)), sem((3, PEERS, SIDE)),
            sem((3, PEERS, SIDE)), sem((3, PEERS, SIDE)),
            sem((3, PEERS)), sem((3, PEERS)), sem((3, PEERS)), sem((3, PEERS)),
        ],
        compiler_params=pltpu.CompilerParams(
            collective_id=0, has_side_effects=True, vmem_limit_bytes=60 * 2**20
        ),
        name="step",
    )(*operands)


def local(
    tokens,
    cache_keys,
    cache_values,
    cum_gates,
    lengths,
    query_weight,
    key_weight,
    value_weight,
    forget_weight,
    out_weight,
    norm_gain,
    norm_bias,
    dense_gate_weight,
    dense_up_weight,
    dense_down_weight,
    dense_scale,
    expert_gate_weight,
    expert_up_weight,
    expert_down_weight,
    routes,
    route_weights,
):
    return step_call(
        lengths,
        tokens,
        cache_keys,
        cache_values,
        jnp.transpose(cum_gates, (0, 2, 1)),
        query_weight,
        key_weight,
        value_weight,
        jnp.transpose(forget_weight),
        out_weight,
        jnp.transpose(routes),
        jnp.transpose(route_weights),
        jnp.transpose(expert_gate_weight),
        jnp.transpose(expert_up_weight),
        expert_down_weight,
        jnp.transpose(dense_gate_weight),
        jnp.transpose(dense_up_weight),
        dense_down_weight,
        dense_scale.reshape(1, -1),
        norm_gain,
        norm_bias,
    )


def solution(mesh):
    return jax.shard_map(
        local,
        mesh=mesh,
        in_specs=(
            P("ep", None),
            P("ep", None, None),
            P("ep", None, None),
            P("ep", None, None),
            P("ep"),
            P(),
            P(),
            P(),
            P(),
            P("ep", None),
            P(),
            P(),
            P(None, "ep"),
            P(None, "ep"),
            P("ep", None),
            P(),
            P(None, "ep"),
            P(None, "ep"),
            P("ep", None),
            P(),
            P(),
        ),
        out_specs=P("ep", None),
        check_vma=False,
    )
```

```python
import functools

import jax
import jax.numpy as jnp
from jax import lax
from jax.experimental import pallas as pl
from jax.experimental.pallas import tpu as pltpu
from jax.sharding import PartitionSpec as P

MESH = pl.DeviceIdType.MESH
F32 = jnp.float32
BF16 = jnp.bfloat16
SIDE = 4
ROWS = 8
WIDTH = 2048
EXPERTS = 8
FFE = 448
FFD = 44
FFP = 512
CHUNKS = ((0, 768), (768, 640), (1408, 640))
REDUCE_CHUNKS = ((0, 768), (768, 512), (1280, 768))
GATHER_ORDER = ((2, 1, 0), (0, 2, 1), (1, 0, 2))
ATTEND = 4
residual_scale = 1.4142135
norm_eps = 1e-05


def norm_rows(values, gain_row, shift_row):
    centre = jnp.mean(values, axis=-1, keepdims=True)
    centred = values - centre
    spread = jnp.mean(centred * centred, axis=-1, keepdims=True)
    return (centred * lax.rsqrt(spread + norm_eps) * gain_row + shift_row).astype(BF16)


def position():
    me = lax.axis_index("ep")
    core = me % 2
    x = (me // 2) % SIDE
    y = (me // (2 * SIDE)) % SIDE
    z = me // (2 * SIDE * SIDE)
    return core, (z, y, x)


def device_at(core, spot):
    z, y, x = spot
    return (((z * SIDE + y) * SIDE + x) * 2 + core,)


def moved(spot, dim, value):
    return tuple(value if d == dim else spot[d] for d in range(3))


def shifted(spot, dim, offset):
    return moved(spot, dim, (spot[dim] + offset + SIDE) % SIDE)


def columns(k):
    return pl.ds(CHUNKS[k][0], CHUNKS[k][1])


def remote(src, dst, send, recv, target):
    return pltpu.make_async_remote_copy(
        src_ref=src, dst_ref=dst, send_sem=send, recv_sem=recv, device_id=target, device_id_type=MESH
    )


def entry_signal(core, spot):
    barrier = pltpu.get_barrier_semaphore()
    for offset in range(SIDE):
        pl.semaphore_signal(
            barrier, inc=1, device_id=device_at(1 - core, shifted(spot, 2, offset)), device_id_type=MESH
        )
    for dim in range(3):
        for offset in range(1, SIDE):
            pl.semaphore_signal(
                barrier, inc=1, device_id=device_at(core, shifted(spot, dim, offset)), device_id_type=MESH
            )


def entry_wait():
    pl.semaphore_wait(pltpu.get_barrier_semaphore(), 3 * (SIDE - 1) + SIDE)


PROJ = 256
HALF = 128
WEIGHT_ORDER = ((1, 0), (0, 1))
NT = (((1,), (1,)), ((), ()))
GROUP = 4
HEAD_LANES = 64
PEERS = SIDE - 1
PIECES = (1, 3, 2)
FAR_FIRST = (2, 1, 3)
LINE = tuple((offset, flip) for offset in FAR_FIRST + (0,) for flip in range(2) if offset or flip)


def spread_heads(pairs):
    lane = lax.broadcasted_iota(jnp.int32, (8, 2 * HEAD_LANES), 1)
    low = lane < HEAD_LANES
    first, second = pairs[:8], pairs[8:]
    return jnp.concatenate(
        [
            jnp.where(low, first, 0.0),
            jnp.where(low, pltpu.roll(first, HEAD_LANES, 1), 0.0),
            jnp.where(low, 0.0, pltpu.roll(second, HEAD_LANES, 1)),
            jnp.where(low, 0.0, second),
        ],
        axis=0,
    )


def pair_heads(heads):
    lane = lax.broadcasted_iota(jnp.int32, (8, 2 * HEAD_LANES), 1)
    low = lane < HEAD_LANES
    first = jnp.where(low, heads[:8], pltpu.roll(heads[8:16], HEAD_LANES, 1))
    second = jnp.where(low, pltpu.roll(heads[16:24], HEAD_LANES, 1), heads[24:])
    return jnp.concatenate([first, second], axis=0)


def attend_some(first, count, lengths_ref, keys_ref, values_ref, gates_ref, pairs_ref, fresh_ref, gate_ref, mixed_ref):
    slots = keys_ref.shape[1]
    place = lax.broadcasted_iota(jnp.int32, (2, slots), 1)
    column = lax.broadcasted_iota(jnp.int32, (2, ROWS), 1)
    state = []
    for step in range(count):
        b = first + step
        queries = spread_heads(pairs_ref[b])
        scores = lax.dot_general(
            queries.astype(BF16), keys_ref[b], NT, preferred_element_type=F32
        )
        length = lengths_ref[b]
        sums = gates_ref[b]
        latest = jnp.sum(jnp.where(place == length - 1, sums, 0.0), axis=1, keepdims=True)
        fresh_gate = jnp.sum(jnp.where(column == b, gate_ref[...], 0.0), axis=1, keepdims=True)
        offsets = jnp.where(place < length, latest - sums + fresh_gate, -jnp.inf)
        wide = jnp.concatenate(
            [jnp.broadcast_to(offsets[:1], (16, slots)), jnp.broadcast_to(offsets[1:], (16, slots))], axis=0
        )
        scores = scores + wide
        fresh = fresh_ref[pl.ds(b, 1), :]
        own = jnp.sum(queries * fresh[:, : 2 * HEAD_LANES], axis=1, keepdims=True)
        state.append((scores, own, fresh[:, 2 * HEAD_LANES :]))
    for step, (scores, own, fresh_value) in enumerate(state):
        b = first + step
        highest = jnp.maximum(jnp.max(scores, axis=1, keepdims=True), own)
        past = jnp.exp(scores - highest)
        own = jnp.exp(own - highest)
        ratio = 1.0 / (jnp.sum(past, axis=1, keepdims=True) + own)
        weights = (past * ratio).astype(BF16)
        own_weight = (own * ratio).astype(BF16).astype(F32)
        mixed = jnp.dot(weights, values_ref[b], preferred_element_type=F32) + own_weight * fresh_value
        mixed_ref[b] = pair_heads(mixed)


class Transfers:
    def __init__(self):
        self.started = []

    def go(self, copy):
        copy.start()
        self.started.append(copy)

    def drain(self):
        for copy in self.started:
            copy.wait_send()
        self.started = []


class Spread:
    def __init__(self, moves, view, core, spot, first, second, send1, recv1, send2, recv2):
        self.moves, self.view, self.core, self.spot = moves, view, core, spot
        self.first, self.second = first, second
        self.send1, self.recv1, self.send2, self.recv2 = send1, recv1, send2, recv2

    def near_copy(self, offset, source, target):
        region = self.view(source)
        return remote(region, region, self.send1.at[offset - 1], self.recv1.at[offset - 1], device_at(self.core, target))

    def far_copy(self, offset, piece, source, target):
        region = self.view(shifted(source, self.first, -piece))
        return remote(
            region, region, self.send2.at[offset - 1, piece], self.recv2.at[offset - 1, piece],
            device_at(self.core, target),
        )

    def far_start(self, piece):
        for offset in FAR_FIRST:
            self.moves.go(self.far_copy(offset, piece, self.spot, shifted(self.spot, self.second, offset)))

    def start(self):
        for offset in PIECES:
            self.moves.go(self.near_copy(offset, self.spot, shifted(self.spot, self.first, offset)))
        self.far_start(0)

    def relay(self, offset):
        self.near_copy(offset, shifted(self.spot, self.first, -offset), self.spot).wait_recv()
        self.far_start(offset)

    def far_arrive(self, offset):
        source = shifted(self.spot, self.second, -offset)
        for piece in range(SIDE):
            self.far_copy(offset, piece, source, self.spot).wait_recv()


def step_kernel(
    lengths_hbm, tokens_hbm, keys_hbm, values_hbm, gates_hbm, query_hbm, key_hbm, value_hbm, forget_hbm, ow_hbm,
    routes_hbm, shares_hbm, gate_hbm, up_hbm, down_hbm, dgate_hbm, dup_hbm, ddown_hbm,
    scale_hbm, gain_hbm, bias_hbm, out_ref,
    lengths_ref, tokens_ref, keys_ref, values_ref, gates_ref, wq_ref, wkv_ref, forget_ref, ow_ref, wo_ref,
    routes_ref, shares_ref, scale_ref, gain_ref, bias_ref,
    pairs_ref, mixed_ref, fresh_ref, newgate_ref, line_ref, sent_ref, back_ref, settled_ref,
    rows_ref, wg_ref, wu_ref, wd_ref, dense_ref, factor_ref, hidden_ref, part_ref, r0_ref, r1_ref, r2_ref, s1_ref, s2_ref,
    asem, wsem, swsend, swrecv, xsend, xrecv, w1send, w1recv, w2send, w2recv,
    lsend, lrecv, bsend, brecv,
    g0send, g0recv, g1send, g1recv, g2send, g2recv,
    rsend, rrecv, r1send, r1recv, r2send, r2recv,
):
    core, spot = position()
    partner = device_at(1 - core, spot)
    entry_signal(core, spot)
    depth = WIDTH // GROUP
    first_loads = [(ow_hbm, ow_ref)]
    small = [
        (tokens_hbm, tokens_ref),
        (forget_hbm, forget_ref),
        (key_hbm, wkv_ref.at[:, pl.ds(0, 128)]),
        (value_hbm, wkv_ref.at[:, pl.ds(128, 128)]),
    ]
    wide = [(query_hbm.at[pl.ds(i * depth, depth)], wq_ref.at[pl.ds(i * depth, depth)]) for i in range(GROUP)]
    cache = [
        (keys_hbm, keys_ref), (values_hbm, values_ref), (gates_hbm, gates_ref), (lengths_hbm, lengths_ref),
        (gain_hbm, gain_ref), (bias_hbm, bias_ref), (scale_hbm, scale_ref),
        (routes_hbm, routes_ref), (shares_hbm, shares_ref),
    ]
    tables = ((gate_hbm, wg_ref), (up_hbm, wu_ref), (down_hbm, wd_ref))
    dense = (dgate_hbm, dup_hbm, ddown_hbm)
    shard = [(hbm, ref.at[core, pl.ds(0, FFE)]) for hbm, ref in tables]
    shard += [(hbm, dense_ref.at[core, i]) for i, hbm in enumerate(dense)]
    count = 0
    groups = []
    for group in (first_loads, small, wide, cache, shard):
        copies = []
        for source, target in group:
            copies.append(pltpu.make_async_copy(source, target, asem.at[count]))
            count += 1
        groups.append(copies)
    first_loads, small, wide, cache, shard = groups
    for load in first_loads + small + wide + cache:
        load.start()

    moves = Transfers()
    me = spot[2] * 2 + core

    def swap_copy(table, part, owner):
        hbm, ref = tables[table]
        size = FFE // 4
        here = pl.ds(part * size, size)
        return remote(
            hbm.at[here], ref.at[owner, here], swsend.at[table * 4 + part], swrecv.at[table * 4 + part], partner
        )

    def swap_dense(i, owner):
        return remote(dense[i], dense_ref.at[owner, i], swsend.at[12 + i], swrecv.at[12 + i], partner)

    def swap_start(table):
        for part in range(4):
            moves.go(swap_copy(table, part, core))
        moves.go(swap_dense(table, core))

    def line_target(offset, flip, sign=1):
        return (core if flip == 0 else 1 - core), shifted(spot, 2, sign * offset)

    def block_copy(index, from_core, source, to_core, target):
        z, y, x = source
        here = pl.multiple_of((target[2] * 2 + to_core) * PROJ, PROJ)
        return remote(
            ow_ref.at[:, pl.ds(here, PROJ)], wo_ref.at[z, y, x, from_core], xsend.at[index], xrecv.at[index],
            device_at(to_core, target),
        )

    for load in first_loads:
        load.wait()
    wo_ref[spot[0], spot[1], spot[2], core] = ow_ref[:, pl.ds(pl.multiple_of(me * PROJ, PROJ), PROJ)]
    entry_wait()
    for index, (offset, flip) in enumerate(LINE):
        moves.go(block_copy(index, core, spot, *line_target(offset, flip)))
    for load in shard:
        load.start()

    def weight_view(k):
        def view(source):
            return wo_ref.at[
                source[0], source[1], pl.ds(0, SIDE), pl.ds(0, 2), pl.ds(0, 2 * ROWS), pl.ds(k * HALF, HALF)
            ]

        return view

    weights = [
        Spread(
            moves, weight_view(k), core, spot, *WEIGHT_ORDER[k],
            w1send.at[k], w1recv.at[k], w2send.at[k], w2recv.at[k],
        )
        for k in range(2)
    ]

    for load in small:
        load.wait()
    tokens = tokens_ref[...]
    fresh_ref[...] = jnp.dot(tokens, wkv_ref[...], preferred_element_type=F32).astype(BF16).astype(F32)
    raw = lax.dot_general(forget_ref[...], tokens, NT, preferred_element_type=F32)
    newgate_ref[...] = jnp.minimum(raw, 0.0) - jnp.log1p(jnp.exp(-jnp.abs(raw)))
    query = jnp.zeros((ROWS, WIDTH), F32)
    for i in range(GROUP):
        wide[i].wait()
        query = query + jnp.dot(
            tokens[:, i * depth : (i + 1) * depth], wq_ref[i * depth : (i + 1) * depth, :], preferred_element_type=F32
        )
    query = query.astype(BF16).astype(F32) * HEAD_LANES**-0.5
    flat = pairs_ref.reshape(ROWS * 16, 128)
    for i in range(16):
        flat[pl.ds(i, ROWS, stride=16), :] = query[:, 128 * i : 128 * (i + 1)]
    for index, (offset, flip) in enumerate(LINE):
        from_core, source = line_target(offset, flip, -1)
        block_copy(index, from_core, source, core, spot).wait_recv()
    for weight in weights:
        weight.start()
    swap_start(0)
    for load in cache:
        load.wait()

    def some(i, carry):
        attend_some(
            i * ATTEND, ATTEND, lengths_ref, keys_ref, values_ref, gates_ref, pairs_ref, fresh_ref, newgate_ref,
            mixed_ref,
        )
        return carry

    lax.fori_loop(0, ROWS // ATTEND, some, 0)
    flat = mixed_ref.reshape(ROWS * 16, 128)
    attended = jnp.concatenate([flat[pl.ds(i, ROWS, stride=16), :] for i in range(16)], axis=1).astype(BF16)
    line_ref[spot[2], core] = attended

    def line_copy(index, from_core, source, to_core, target):
        here = line_ref.at[source[2], from_core]
        return remote(here, here, lsend.at[index], lrecv.at[index], device_at(to_core, target))

    for index, (offset, flip) in enumerate(LINE):
        moves.go(line_copy(index, core, spot, *line_target(offset, flip)))
    for offset in PIECES:
        for weight in weights:
            weight.relay(offset)
    swap_start(1)
    swap_start(2)

    expert = lax.axis_index("ep") // (2 * SIDE * SIDE * SIDE // EXPERTS)
    picked = jnp.where(routes_ref[...] == expert, shares_ref[...], 0.0)
    factor = jnp.sum(picked, axis=0, keepdims=True)
    turned = jnp.transpose(jnp.broadcast_to(factor, (8, factor.shape[1])))
    factor_ref[...] = turned.reshape(factor_ref.shape)

    for index, (offset, flip) in enumerate(LINE):
        from_core, source = line_target(offset, flip, -1)
        line_copy(index, from_core, source, core, spot).wait_recv()
    for offset in PIECES:
        for weight in weights:
            weight.far_arrive(offset)
    lines = line_ref.reshape(2 * SIDE * ROWS, WIDTH)[...]
    sent_ref.reshape(2 * SIDE * ROWS, PROJ)[...] = jnp.dot(
        lines, wo_ref.reshape(WIDTH, PROJ)[...], preferred_element_type=F32
    )

    def back_copy(index, from_core, source, to_core, target):
        return remote(
            sent_ref.at[target[2], to_core], back_ref.at[source[2], from_core], bsend.at[index], brecv.at[index],
            device_at(to_core, target),
        )

    for index, (offset, flip) in enumerate(LINE):
        moves.go(back_copy(index, core, spot, *line_target(offset, flip)))
    back_ref[spot[2], core] = sent_ref[spot[2], core]
    for index, (offset, flip) in enumerate(LINE):
        from_core, source = line_target(offset, flip, -1)
        back_copy(index, from_core, source, core, spot).wait_recv()
    projected = jnp.concatenate([back_ref[i // 2, i % 2] for i in range(2 * SIDE)], axis=1)
    settled = norm_rows(residual_scale * tokens.astype(F32) + projected, gain_ref[0:1, :], bias_ref[0:1, :])
    settled_ref[...] = settled
    rows_ref[spot] = settled

    def row_view(k):
        gone = GATHER_ORDER[k][0]

        def view(source):
            where = tuple(pl.ds(0, SIDE) if d == gone else source[d] for d in range(3))
            return rows_ref.at[where + (pl.ds(0, ROWS), columns(k))]

        return view

    def first_copy(k, offset, source, target):
        region = rows_ref.at[source + (pl.ds(0, ROWS), columns(k))]
        return remote(region, region, g0send.at[k, offset - 1], g0recv.at[k, offset - 1], device_at(core, target))

    for offset in FAR_FIRST:
        for k in range(3):
            moves.go(first_copy(k, offset, spot, shifted(spot, GATHER_ORDER[k][0], offset)))

    pad = jnp.zeros((FFP - FFE - FFD, WIDTH), BF16)

    def dense_rows(slot):
        for i, ref in ((0, wg_ref), (1, wu_ref), (2, wd_ref)):
            value = dense_ref[slot, i]
            if i == 2:
                value = (value.astype(F32) * scale_ref[...]).astype(BF16)
            ref[slot, FFE:, :] = jnp.concatenate([value, pad], axis=0)

    for load in shard:
        load.wait()
    dense_rows(core)
    spreads = [
        Spread(
            moves, row_view(k), core, spot, *GATHER_ORDER[k][1:],
            g1send.at[k], g1recv.at[k], g2send.at[k], g2recv.at[k],
        )
        for k in range(3)
    ]
    for k in range(3):
        for offset in PIECES:
            first_copy(k, offset, shifted(spot, GATHER_ORDER[k][0], -offset), spot).wait_recv()
        spreads[k].start()
    for offset in PIECES:
        for k in range(3):
            spreads[k].relay(offset)
    for table in range(3):
        for part in range(4):
            swap_copy(table, part, 1 - core).wait_recv()
        swap_dense(table, 1 - core).wait_recv()
    dense_rows(1 - core)
    for offset in PIECES:
        for k in range(3):
            spreads[k].far_arrive(offset)

    plane_rows = SIDE * SIDE * ROWS
    block = 2 * plane_rows
    lane = lax.broadcasted_iota(jnp.int32, (1, 2 * FFP), 1) % FFP
    wg_all, wu_all, wd_all = (ref.reshape(2 * FFP, WIDTH) for ref in (wg_ref, wu_ref, wd_ref))

    def plane(offset):
        return shifted(spot, 0, offset)[0]

    def hidden_block(i, carry):
        pair = (plane(2 + i), plane(1 - i))
        x = jnp.concatenate([rows_ref.at[p].reshape(plane_rows, WIDTH)[...] for p in pair], axis=0)
        gate = lax.dot_general(x, wg_all[...], NT, preferred_element_type=F32)
        up = lax.dot_general(x, wu_all[...], NT, preferred_element_type=F32)
        weight = jnp.concatenate(
            [factor_ref[pl.ds(p * SIDE * SIDE, SIDE * SIDE), core].reshape(plane_rows, 8)[:, :1] for p in pair], axis=0
        )
        weight = jnp.where(lane < FFE, weight, 1.0)
        hidden_ref[...] = (gate * jax.nn.sigmoid(gate) * up * weight).astype(BF16)
        return carry

    def down(i, k):
        here = span(k)
        value = jnp.dot(hidden_ref[...], wd_all[:, here], preferred_element_type=F32).astype(BF16)
        for n, p in enumerate((plane(2 + i), plane(1 - i))):
            part_ref.at[p].reshape(plane_rows, WIDTH)[:, here] = value[n * plane_rows : (n + 1) * plane_rows]

    def span(k):
        return pl.ds(REDUCE_CHUNKS[k][0], REDUCE_CHUNKS[k][1])

    def dims_of(k):
        return GATHER_ORDER[k][::-1]

    def cell(ref, lead, k, phase, fixed):
        gone = dims_of(k)[:phase]
        where = tuple(fixed.get(d, pl.ds(0, SIDE)) for d in range(3) if d not in gone)
        return ref.at[lead + where + (pl.ds(0, ROWS), span(k))]

    def send0(k, offset, piece, target):
        a, b, _ = dims_of(k)
        line = (spot[b] + piece) % SIDE
        return remote(
            cell(part_ref, (), k, 0, {a: target[a], b: line}), cell(r0_ref, (offset - 1,), k, 1, {b: line}),
            rsend.at[k, offset - 1, piece], rrecv.at[k, offset - 1, piece], device_at(core, target),
        )

    def send1(k, offset, target):
        b = dims_of(k)[1]
        return remote(
            cell(s1_ref, (), k, 1, {b: target[b]}), cell(r1_ref, (offset - 1,), k, 2, {}),
            r1send.at[k, offset - 1], r1recv.at[k, offset - 1], device_at(core, target),
        )

    def send2(k, offset, target):
        c = dims_of(k)[2]
        return remote(
            cell(s2_ref, (), k, 2, {c: target[c]}), cell(r2_ref, (offset - 1,), k, 3, {}),
            r2send.at[k, offset - 1], r2recv.at[k, offset - 1], device_at(core, target),
        )

    def send_part(k, offsets, pieces):
        for piece in pieces:
            for offset in offsets:
                moves.go(send0(k, offset, piece, shifted(spot, dims_of(k)[0], offset)))

    def sum_part(k, piece):
        a, b, _ = dims_of(k)
        line = (spot[b] + piece) % SIDE
        total = cell(part_ref, (), k, 0, {a: spot[a], b: line})[...].astype(F32)
        for offset in PIECES:
            send0(k, offset, piece, spot).wait_recv()
            total = total + cell(r0_ref, (offset - 1,), k, 1, {b: line})[...].astype(F32)
        cell(s1_ref, (), k, 1, {b: line})[...] = total.astype(BF16)
        if piece:
            moves.go(send1(k, piece, shifted(spot, b, piece)))

    order = (2, 1, 3, 0)
    before = len(moves.started)
    hidden_block(0, 0)
    down(0, 0)
    send_part(0, (2, 1), order)
    down(0, 2)
    send_part(2, FAR_FIRST, (2, 1))
    down(0, 1)
    hidden_block(1, 0)
    down(1, 1)
    send_part(1, FAR_FIRST, order)
    down(1, 0)
    send_part(0, (3,), order)
    down(1, 2)
    early = moves.started[:before]
    moves.started = moves.started[before:]
    send_part(2, FAR_FIRST, (3, 0))
    for copy in early:
        copy.wait_send()
    for k, piece in ((2, 2), (2, 1), (1, 2), (1, 1), (0, 2), (0, 1), (1, 3), (0, 3), (2, 3), (1, 0), (0, 0), (2, 0)):
        sum_part(k, piece)
    for k in range(3):
        b, c = dims_of(k)[1:]
        total = cell(s1_ref, (), k, 1, {b: spot[b]})[...].astype(F32)
        for offset in PIECES:
            send1(k, offset, spot).wait_recv()
            total = total + cell(r1_ref, (offset - 1,), k, 2, {})[...].astype(F32)
        cell(s2_ref, (), k, 2, {})[...] = total.astype(BF16)
        for offset in FAR_FIRST:
            moves.go(send2(k, offset, shifted(spot, c, offset)))
    moves.drain()
    sums = []
    for k in range(3):
        c = dims_of(k)[2]
        total = cell(s2_ref, (), k, 2, {c: spot[c]})[...].astype(F32)
        for offset in PIECES:
            send2(k, offset, spot).wait_recv()
            total = total + cell(r2_ref, (offset - 1,), k, 3, {})[...].astype(F32)
        sums.append(total)
    ffn_sum = jnp.concatenate(sums, axis=-1)
    settled_ref[...] = norm_rows(
        residual_scale * settled_ref[...].astype(F32) + ffn_sum, gain_ref[1:2, :], bias_ref[1:2, :]
    )
    last = pltpu.make_async_copy(settled_ref, out_ref, wsem.at[0])
    last.start()
    moves.drain()
    last.wait()


def step_call(*operands):
    vmem = pl.BlockSpec(memory_space=pltpu.VMEM)
    hbm = pl.BlockSpec(memory_space=pltpu.HBM)
    sem = pltpu.SemaphoreType.DMA
    cube = (SIDE, SIDE, SIDE, ROWS, WIDTH)
    slots = operands[2].shape[1]
    line = len(LINE)
    return pl.pallas_call(
        step_kernel,
        out_shape=jax.ShapeDtypeStruct((ROWS, WIDTH), BF16),
        in_specs=[hbm] * len(operands),
        out_specs=hbm,
        scratch_shapes=[
            pltpu.SMEM((ROWS,), jnp.int32),
            pltpu.VMEM((ROWS, WIDTH), BF16),
            pltpu.VMEM((ROWS, slots, 128), BF16),
            pltpu.VMEM((ROWS, slots, 128), BF16),
            pltpu.VMEM((ROWS, 2, slots), F32),
            pltpu.VMEM((WIDTH, WIDTH), BF16),
            pltpu.VMEM((WIDTH, 256), BF16),
            pltpu.VMEM((2, WIDTH), BF16),
            pltpu.VMEM((2 * ROWS, WIDTH), BF16),
            pltpu.VMEM((SIDE, SIDE, SIDE, 2, 2 * ROWS, PROJ), BF16),
            pltpu.VMEM((2, 2 * SIDE**3 * ROWS), jnp.int32),
            pltpu.VMEM((2, 2 * SIDE**3 * ROWS), F32),
            pltpu.VMEM((1, WIDTH), F32),
            pltpu.VMEM((2, WIDTH), F32),
            pltpu.VMEM((2, WIDTH), F32),
            pltpu.VMEM((ROWS, 16, 128), F32),
            pltpu.VMEM((ROWS, 16, 128), F32),
            pltpu.VMEM((ROWS, 256), F32),
            pltpu.VMEM((2, ROWS), F32),
            pltpu.VMEM((SIDE, 2, ROWS, WIDTH), BF16),
            pltpu.VMEM((SIDE, 2, ROWS, PROJ), F32),
            pltpu.VMEM((SIDE, 2, ROWS, PROJ), F32),
            pltpu.VMEM((ROWS, WIDTH), BF16),
            pltpu.VMEM(cube, BF16),
            pltpu.VMEM((2, FFP, WIDTH), BF16),
            pltpu.VMEM((2, FFP, WIDTH), BF16),
            pltpu.VMEM((2, FFP, WIDTH), BF16),
            pltpu.VMEM((2, 3, FFD, WIDTH), BF16),
            pltpu.VMEM((SIDE**3, 2, ROWS, 8), F32),
            pltpu.VMEM((2 * SIDE * SIDE * ROWS, 2 * FFP), BF16),
            pltpu.VMEM(cube, BF16),
            pltpu.VMEM((PEERS,) + cube[1:], BF16),
            pltpu.VMEM((PEERS,) + cube[2:], BF16),
            pltpu.VMEM((PEERS,) + cube[3:], BF16),
            pltpu.VMEM(cube[1:], BF16),
            pltpu.VMEM(cube[2:], BF16),
            sem((24,)), sem((1,)), sem((15,)), sem((15,)),
            sem((line,)), sem((line,)),
            sem((2, PEERS)), sem((2, PEERS)), sem((2, PEERS, SIDE)), sem((2, PEERS, SIDE)),
            sem((line,)), sem((line,)), sem((line,)), sem((line,)),
            sem((3, PEERS)), sem((3, PEERS)),
            sem((3, PEERS)), sem((3, PEERS)), sem((3, PEERS, SIDE)), sem((3, PEERS, SIDE)),
            sem((3, PEERS, SIDE)), sem((3, PEERS, SIDE)),
            sem((3, PEERS)), sem((3, PEERS)), sem((3, PEERS)), sem((3, PEERS)),
        ],
        compiler_params=pltpu.CompilerParams(
            collective_id=0, has_side_effects=True, vmem_limit_bytes=60 * 2**20
        ),
        name="step",
    )(*operands)


def local(
    tokens,
    cache_keys,
    cache_values,
    cum_gates,
    lengths,
    query_weight,
    key_weight,
    value_weight,
    forget_weight,
    out_weight,
    norm_gain,
    norm_bias,
    dense_gate_weight,
    dense_up_weight,
    dense_down_weight,
    dense_scale,
    expert_gate_weight,
    expert_up_weight,
    expert_down_weight,
    routes,
    route_weights,
):
    return step_call(
        lengths,
        tokens,
        cache_keys,
        cache_values,
        jnp.transpose(cum_gates, (0, 2, 1)),
        query_weight,
        key_weight,
        value_weight,
        jnp.transpose(forget_weight),
        out_weight,
        jnp.transpose(routes),
        jnp.transpose(route_weights),
        jnp.transpose(expert_gate_weight),
        jnp.transpose(expert_up_weight),
        expert_down_weight,
        jnp.transpose(dense_gate_weight),
        jnp.transpose(dense_up_weight),
        dense_down_weight,
        dense_scale.reshape(1, -1),
        norm_gain,
        norm_bias,
    )


def solution(mesh):
    return jax.shard_map(
        local,
        mesh=mesh,
        in_specs=(
            P("ep", None),
            P("ep", None, None),
            P("ep", None, None),
            P("ep", None, None),
            P("ep"),
            P(),
            P(),
            P(),
            P(),
            P("ep", None),
            P(),
            P(),
            P(None, "ep"),
            P(None, "ep"),
            P("ep", None),
            P(),
            P(None, "ep"),
            P(None, "ep"),
            P("ep", None),
            P(),
            P(),
        ),
        out_specs=P("ep", None),
        check_vma=False,
    )
```
